32 devices in a mesh: ep: 4 (over y, x), tp: 8 (over z, core).
Axes of the slice: x: 2, y: 2, z: 4, core: 2. Of those that a mesh axis runs over, the one named last changes fastest.
Arguments:
- tokens: bfloat16 [768, 2048], P('ep'), may hold values from -6 to 6
- cotangent: bfloat16 [768, 2048], P('ep'), may hold values from -6 to 6
- routes: int32 [768, 2], P('ep'), may hold values from 0 to 3, all different within a row; in each aligned block of 192 rows (0 to 191, 192 to 383, ...) at most 192 rows name the same one
- route_weight: float32 [768, 2], P('ep'), may hold values from 0.2 to 1
- gate_weight: bfloat16 [4, 2048, 4096], P('ep', None, 'tp'), may hold values from -0.125 to 0.125
- up_weight: bfloat16 [4, 2048, 4096], P('ep', None, 'tp'), may hold values from -0.125 to 0.125
- down_weight: bfloat16 [4, 4096, 2048], P('ep', 'tp'), may hold values from -0.09375 to 0.09375
Outputs:
- grad_tokens: bfloat16 [768, 2048], P('ep', 'tp')
- grad_route: float32 [768, 2], P('ep')
- grad_gate: bfloat16 [4, 2048, 4096], P('ep', None, 'tp')
- grad_up: bfloat16 [4, 2048, 4096], P('ep', None, 'tp')
- grad_down: bfloat16 [4, 4096, 2048], P('ep', 'tp')
The draws below stay inside these ranges and needn't reach their ends.
Inputs may be any that keep to these rules, and one draw needn't show every extreme that they name: `routes`: within the rows of one device along ep, each expert is named at most 192 times, a bound that some block reaches; the 2 entries of a row differ.
All inputs are finite; a program needn't handle non-finite values.
Results may differ from the reference program's by a relative error of at most 0.025.
Values may be sent and summed in bfloat16 or wider, within the bound.
A program may use at most 64 MiB of HBM per device.

```python
import math
import jax
import jax.numpy as jnp
import numpy as np
from jax import lax

D = 2048
FF = 4096
TOP = 2
TOK_DEV = 192
EXPERTS = 4
TOKENS = 768
CAP = 192
N_EP = 4
N_TP = 8


def shard_levels(key, extent, shards, least, largest):
    loudness, own = 1.0, jax.random.fold_in(key, 6)
    for axis_at, blocks in shards:
        steps = jnp.exp(jax.random.uniform(jax.random.fold_in(own, axis_at), (blocks,), jnp.float32, least / len(shards), largest / len(shards)))
        loudness = loudness * jnp.repeat(steps, extent[axis_at] // blocks).reshape([-1 if axis == axis_at else 1 for axis in range(len(extent))])
    return loudness


def assign_block(rng, own, number, rows, count, top, reach, lean):
    ranking = jax.random.permutation(rng, count)
    crowded, usual = shares(count, rows * top, reach, lean, True), shares(count, rows * top, reach, lean, False)
    places = jnp.arange(count)

    def named(sizes, turn):
        used = int((sizes > 0).sum())
        fixed = max(1, used // 4)
        passed = fixed + (places - fixed + turn * (used - fixed)) % max(1, count - fixed)
        return jnp.zeros((count,), jnp.int32).at[ranking[jnp.where(places < fixed, places, passed)]].set(jnp.asarray(sizes, jnp.int32))

    sizes = jnp.where(number % 4 == 0, named(crowded, number // 4), named(usual, number - number // 4 - 1))
    mixed = jax.random.permutation(jax.random.fold_in(own, 3), count)
    source_of, taker = mixed[0:count // 2 * 2:2], mixed[1:count // 2 * 2:2]
    slack = jnp.minimum(sizes[source_of] - 1, reach - sizes[taker]) // 2
    slack = jnp.where((source_of == ranking[0]) | (taker == ranking[0]) | (sizes[taker] == 0), 0, jnp.maximum(slack, 0))
    passed = jax.random.randint(jax.random.fold_in(own, 4), (count // 2,), 0, 1 << 20) % (slack + 1)
    sizes = sizes.at[source_of].add(-passed).at[taker].add(passed)
    items = jnp.searchsorted(jnp.cumsum(sizes), jnp.arange(rows * top), side="right").astype(jnp.int32)
    listing = items.reshape(top, rows).T
    listing = listing[jax.random.permutation(jax.random.fold_in(own, 1), rows)]
    turn = jax.random.randint(jax.random.fold_in(own, 2), (rows, 1), 0, top)
    return jnp.take_along_axis(listing, (jnp.arange(top)[None, :] + turn) % top, axis=1)


def shares(count, total, reach, slope, full):
    weights = [(1 << 20) // math.isqrt(grade ** slope) + 1 for grade in range(1, count + 1)]
    largest = reach if full else min(reach, max(-(-total // count), total * weights[0] // sum(weights)))
    least = 1 if total - largest >= count - 1 else 0
    holding, rest = [largest] + [least] * (count - 1), total - largest - least * (count - 1)
    while rest > 0:
        candidates = [i for i in range(1, count) if holding[i] < largest] or [i for i in range(1, count) if holding[i] < reach]
        whole, remaining = sum([weights[i] for i in candidates]), rest
        for i in candidates:
            addition = min(reach - holding[i], max(1, remaining * weights[i] // whole), rest)
            holding[i] = holding[i] + addition
            rest = rest - addition
    return np.array(holding)


def gaussian(own_key, shape, deviation, most, cuts=(), kind=jnp.bfloat16):
    array = jax.random.normal(own_key, shape, jnp.float32) * deviation
    if len(cuts) > 0:
        array = shard_levels(own_key, shape, cuts, -0.22, 0.18) * array
    return jnp.clip(array, min=-most, max=most).astype(kind)


def setup_inputs(seed: int = 0) -> dict:
    seeds = jax.random.split(jax.random.key(seed), 8)
    tokens = gaussian(seeds[0], (TOKENS, D), 1.0, 6.0, ((0, 4),))
    cotangent = gaussian(seeds[1], (TOKENS, D), 1.0, 6.0, ((0, 4),))
    routes_keys = jax.random.split(jax.random.fold_in(seeds[2], 1), TOKENS // TOK_DEV)
    routes_turns = jax.random.permutation(jax.random.fold_in(seeds[2], 3), TOKENS // TOK_DEV)
    routes = jax.vmap(lambda own, number: assign_block(jax.random.fold_in(seeds[2], 2), own, number, TOK_DEV, EXPERTS, TOP, CAP, 2))(routes_keys, routes_turns).reshape((TOKENS, TOP))
    route_weight = jnp.clip(0.2 + 0.8 * jax.random.uniform(seeds[3], (TOKENS, TOP), jnp.float32) ** shard_levels(seeds[3], (TOKENS, TOP), ((0, 4),), -0.2, 0.2), 0.2, 1.0)
    gate_weight = gaussian(seeds[4], (EXPERTS, D, FF), D ** -0.5, 0.125, ((0, 4), (2, 8)))
    up_weight = gaussian(seeds[5], (EXPERTS, D, FF), D ** -0.5, 0.125, ((0, 4), (2, 8)))
    down_weight = gaussian(seeds[6], (EXPERTS, FF, D), FF ** -0.5, 0.09375, ((0, 4), (1, 8)))
    return dict(tokens=tokens, cotangent=cotangent, routes=routes, route_weight=route_weight, gate_weight=gate_weight, up_weight=up_weight, down_weight=down_weight)


def slot_layout(routes):
    flat_routes = routes.reshape(N_EP, TOK_DEV * TOP).astype(jnp.int32)
    expert_ids = jnp.arange(EXPERTS, dtype=jnp.int32)
    onehot_table = (flat_routes[:, :, None] == expert_ids[None, None, :]).astype(jnp.int32)
    earlier = jnp.cumsum(onehot_table, axis=1) - onehot_table
    order_in = jnp.sum(earlier * onehot_table, axis=2).astype(jnp.int32)
    source_block = jnp.arange(N_EP, dtype=jnp.int32)[:, None]
    position = (source_block * CAP + order_in).astype(jnp.int32)
    entries = jnp.arange(N_EP * TOK_DEV * TOP, dtype=jnp.int32).reshape(N_EP, TOK_DEV * TOP) + 1
    slot_table = jnp.zeros((EXPERTS, N_EP * CAP), jnp.int32).at[flat_routes, position].set(entries)
    return slot_table


def expert_step(x_rows, c_rows, w_rows, w_gate, w_upper, w_lower):
    gate_pre = jnp.dot(x_rows, w_gate, preferred_element_type=jnp.float32)
    up_pre = jnp.dot(x_rows, w_upper, preferred_element_type=jnp.float32)
    sig = jax.nn.sigmoid(gate_pre)
    active = gate_pre * sig
    hidden = (active * up_pre).astype(jnp.bfloat16)
    back_raw = jnp.dot(c_rows, w_lower.T, preferred_element_type=jnp.float32)
    route_part = jnp.sum(hidden.astype(jnp.float32) * back_raw, axis=1)
    scaled_back = w_rows[:, None] * back_raw
    grad_gate_pre = (scaled_back * up_pre * sig * (1.0 + gate_pre * (1.0 - sig))).astype(jnp.bfloat16)
    grad_up_pre = (scaled_back * active).astype(jnp.bfloat16)
    scaled_cot = (w_rows[:, None] * c_rows.astype(jnp.float32)).astype(jnp.bfloat16)
    grad_wg = jnp.dot(x_rows.T, grad_gate_pre, preferred_element_type=jnp.float32).astype(jnp.bfloat16)
    grad_wu = jnp.dot(x_rows.T, grad_up_pre, preferred_element_type=jnp.float32).astype(jnp.bfloat16)
    grad_wd = jnp.dot(hidden.T, scaled_cot, preferred_element_type=jnp.float32).astype(jnp.bfloat16)
    group_width = FF // N_TP

    def add_group(group, total):
        lower = (group * group_width).astype(jnp.int32)
        part = jnp.dot(lax.dynamic_slice_in_dim(grad_gate_pre, lower, group_width, 1),
                       lax.dynamic_slice_in_dim(w_gate, lower, group_width, 1).T,
                       preferred_element_type=jnp.float32)
        part = part + jnp.dot(lax.dynamic_slice_in_dim(grad_up_pre, lower, group_width, 1),
                              lax.dynamic_slice_in_dim(w_upper, lower, group_width, 1).T,
                              preferred_element_type=jnp.float32)
        return total + lax.optimization_barrier(part.astype(jnp.bfloat16)).astype(jnp.float32)

    start_total = jnp.zeros((x_rows.shape[0], D), jnp.float32)
    row_total = lax.fori_loop(jnp.int32(0), jnp.int32(N_TP), add_group, start_total)
    return grad_wg, grad_wu, grad_wd, row_total.astype(jnp.bfloat16), route_part


def reference(tokens, cotangent, routes, route_weight, gate_weight, up_weight, down_weight):
    slot_table = slot_layout(routes)
    filled = slot_table > 0
    entry = jnp.maximum(slot_table - 1, 0).astype(jnp.int32)
    flat_weight = route_weight.reshape(-1)

    def per_expert(args):
        filled_e, entry_e, w_gate, w_upper, w_lower = args
        source_row = (entry_e // TOP).astype(jnp.int32)
        x_rows = jnp.where(filled_e[:, None], tokens[source_row], jnp.zeros((), jnp.bfloat16)).astype(jnp.bfloat16)
        c_rows = jnp.where(filled_e[:, None], cotangent[source_row], jnp.zeros((), jnp.bfloat16)).astype(jnp.bfloat16)
        w_round = jnp.where(filled_e, flat_weight[entry_e], jnp.zeros((), jnp.float32)).astype(jnp.bfloat16)
        w_rows = lax.optimization_barrier(w_round).astype(jnp.float32)
        return expert_step(x_rows, c_rows, w_rows, w_gate, w_upper, w_lower)

    grad_gate, grad_up, grad_down, row_grads, route_parts = lax.map(
        per_expert, (filled, entry, gate_weight, up_weight, down_weight))
    target = jnp.where(filled, slot_table - 1, TOKENS * TOP).astype(jnp.int32).reshape(-1)
    flat_rows = jnp.zeros((TOKENS * TOP, D), jnp.bfloat16).at[target].set(row_grads.reshape(-1, D), mode="drop")
    grad_tokens = jnp.sum(flat_rows.reshape(TOKENS, TOP, D).astype(jnp.float32), axis=1).astype(jnp.bfloat16)
    flat_route = jnp.zeros((TOKENS * TOP,), jnp.float32).at[target].set(route_parts.reshape(-1), mode="drop")
    grad_route = flat_route.reshape(TOKENS, TOP)
    return grad_tokens, grad_route, grad_gate, grad_up, grad_down
```

```python
import functools

import jax
import jax.numpy as jnp
from jax import lax
from jax.experimental import pallas as pl
from jax.experimental.pallas import tpu as pltpu
from jax.sharding import PartitionSpec as P

F32, BF16 = jnp.float32, jnp.bfloat16
LANES = 256
CHUNKS = 2
VLIM = 40


def shards(tokens, cotangent, routes, route_weight, gate_weight, up_weight, down_weight):
    rows, model_width = tokens.shape
    top = routes.shape[1]
    local_experts = gate_weight.shape[0]
    experts_all = local_experts * lax.axis_size("ep")
    capacity = 2 * rows * top // experts_all
    shard_width = model_width // lax.axis_size("tp")
    flat_routes = routes.reshape(-1)
    expert_ids = jnp.arange(experts_all, dtype=jnp.int32)
    onehot_table = (flat_routes[:, None] == expert_ids[None, :]).astype(jnp.int32)
    earlier = jnp.cumsum(onehot_table, axis=0) - onehot_table
    order_in = jnp.sum(earlier * onehot_table, axis=1)
    slot_index = flat_routes * capacity + order_in
    entries = jnp.arange(rows * top, dtype=jnp.int32) + 1
    slot_table = jnp.zeros((experts_all * capacity,), jnp.int32).at[slot_index].set(entries)
    filled = slot_table > 0
    entry = jnp.maximum(slot_table - 1, 0)
    source_row = entry // top
    zero_value = jnp.zeros((), jnp.bfloat16)
    token_buf = jnp.where(filled[:, None], tokens[source_row], zero_value).reshape(
        experts_all, capacity, model_width
    )
    cot_buf = jnp.where(filled[:, None], cotangent[source_row], zero_value).reshape(
        experts_all, capacity, model_width
    )
    weight_buf = (
        jnp.where(filled, route_weight.reshape(-1)[entry], 0.0)
        .astype(jnp.bfloat16)
        .reshape(experts_all, capacity)
    )
    start = lax.axis_index("tp") * shard_width
    token_part = lax.dynamic_slice_in_dim(token_buf, start, shard_width, 2)
    cot_part = lax.dynamic_slice_in_dim(cot_buf, start, shard_width, 2)
    token_part, cot_part, arrived_weight = (
        lax.all_to_all(token_part, "ep", split_axis=0, concat_axis=1, tiled=True),
        lax.all_to_all(cot_part, "ep", split_axis=0, concat_axis=1, tiled=True),
        lax.all_to_all(weight_buf, "ep", split_axis=0, concat_axis=1, tiled=True),
    )
    arrived_tokens, arrived_cot = (
        lax.all_gather(token_part, "tp", axis=2, tiled=True),
        lax.all_gather(cot_part, "tp", axis=2, tiled=True),
    )
    gate_pre = jnp.einsum(
        "erd,edf->erf", arrived_tokens, gate_weight, preferred_element_type=jnp.float32
    )
    up_pre = jnp.einsum(
        "erd,edf->erf", arrived_tokens, up_weight, preferred_element_type=jnp.float32
    )
    sig = jax.nn.sigmoid(gate_pre)
    active = gate_pre * sig
    hidden = (active * up_pre).astype(jnp.bfloat16)
    back_raw = jnp.einsum(
        "erd,efd->erf", arrived_cot, down_weight, preferred_element_type=jnp.float32
    )
    route_part = jnp.sum(hidden.astype(jnp.float32) * back_raw, axis=2)
    slot_weight = arrived_weight.astype(jnp.float32)
    scaled_back = slot_weight[:, :, None] * back_raw
    grad_gate_pre = (scaled_back * up_pre * sig * (1.0 + gate_pre * (1.0 - sig))).astype(
        jnp.bfloat16
    )
    grad_up_pre = (scaled_back * active).astype(jnp.bfloat16)
    scaled_cot = (slot_weight[:, :, None] * arrived_cot).astype(jnp.bfloat16)
    grad_gate = jnp.einsum(
        "erd,erf->edf", arrived_tokens, grad_gate_pre, preferred_element_type=jnp.float32
    ).astype(jnp.bfloat16)
    grad_up = jnp.einsum(
        "erd,erf->edf", arrived_tokens, grad_up_pre, preferred_element_type=jnp.float32
    ).astype(jnp.bfloat16)
    grad_down = jnp.einsum(
        "erf,erd->efd", hidden, scaled_cot, preferred_element_type=jnp.float32
    ).astype(jnp.bfloat16)
    row_part = jnp.einsum(
        "erf,edf->erd", grad_gate_pre, gate_weight, preferred_element_type=jnp.float32
    )
    row_part = row_part + jnp.einsum(
        "erf,edf->erd", grad_up_pre, up_weight, preferred_element_type=jnp.float32
    )
    row_summed = lax.psum_scatter(
        row_part.astype(jnp.bfloat16), "tp", scatter_dimension=2, tiled=True
    )
    returned = lax.all_to_all(row_summed, "ep", split_axis=1, concat_axis=0, tiled=True)
    route_total = lax.psum(route_part, "tp")
    route_back = lax.all_to_all(route_total, "ep", split_axis=1, concat_axis=0, tiled=True)
    per_entry = returned.reshape(experts_all * capacity, shard_width)[slot_index]
    grad_tokens = jnp.sum(
        per_entry.astype(jnp.float32).reshape(rows, top, shard_width), axis=1
    ).astype(jnp.bfloat16)
    grad_route = route_back.reshape(-1)[slot_index].reshape(rows, top)
    return (grad_tokens, grad_route, grad_gate, grad_up, grad_down)


def step_kernel(
    n_ep, n_tp,
    x_hbm, c_hbm, routes_hbm, weight_hbm, wg_hbm, wu_hbm, wd_hbm,
    gt_ref, rt_ref, gg, gu, gd,
    routes_ref, weight_ref, xc, wt, wg, wu, wd, hid, da, db, sc, rp, pr, r1, r2, zr, rcol, rm, rr, ra, rb,
    lsem, s_fwd, r_fwd, s_pair, r_pair, s_rp, r_rp, s_xy, r_xy, s_z, r_z, s_rt, r_rt,
):
    nz = n_tp // 2
    hz = nz // 2
    rows, width = x_hbm.shape
    hidden_units = wg.shape[1]
    shard = width // n_tp
    piece = rows // (nz + 2)
    unit = rows // CHUNKS
    p, t = lax.axis_index("ep"), lax.axis_index("tp")
    k, z = t % 2, t // 2
    px, py, pd = p + 1 - 2 * (p % 2), p + 2 - 4 * (p // 2), 3 - p
    mate = t + 1 - 2 * k

    def remote(src, dst, send, recv, ep, tp):
        return pltpu.make_async_remote_copy(
            src_ref=src, dst_ref=dst, send_sem=send, recv_sem=recv,
            device_id={"ep": ep, "tp": tp}, device_id_type=pl.DeviceIdType.MESH,
        )

    local = [
        pltpu.make_async_copy(x_hbm, xc.at[p, pl.ds(0, rows)], lsem.at[0]),
        pltpu.make_async_copy(c_hbm, xc.at[p, pl.ds(rows, rows)], lsem.at[1]),
        pltpu.make_async_copy(routes_hbm, routes_ref, lsem.at[5]),
        pltpu.make_async_copy(weight_hbm, weight_ref, lsem.at[6]),
        pltpu.make_async_copy(wg_hbm, wg, lsem.at[2]),
        pltpu.make_async_copy(wu_hbm, wu, lsem.at[3]),
        pltpu.make_async_copy(wd_hbm, wd, lsem.at[4]),
    ]
    for copy in local:
        copy.start()
    barrier = pltpu.get_barrier_semaphore()
    for other in (px, py, pd):
        pl.semaphore_signal(barrier, inc=1, device_id={"ep": other, "tp": t}, device_id_type=pl.DeviceIdType.MESH)
    for step in range(1, n_tp):
        pl.semaphore_signal(barrier, inc=1, device_id={"ep": p, "tp": (t + step) % n_tp}, device_id_type=pl.DeviceIdType.MESH)
    for copy in local[2:4]:
        copy.wait()
    experts = lax.broadcasted_iota(jnp.int32, (8, rows), 0)
    mixed = jnp.zeros((8, rows), F32)
    for choice in range(routes_ref.shape[0]):
        hit = routes_ref[choice:choice + 1, :] == experts
        mixed = mixed + jnp.where(hit, weight_ref[choice:choice + 1, :], 0.0)
    wt[p] = jnp.zeros(wt.shape[1:], F32)
    wt[p, :, 0:rows] = mixed.astype(BF16).astype(F32)
    pl.semaphore_wait(barrier, n_ep - 1 + n_tp - 1)
    for copy in local[:2]:
        copy.wait()

    sends = []

    def go(copy):
        copy.start()
        sends.append(copy)

    def sub_rows(half, lower, count):
        return pl.ds(pl.multiple_of(half * rows + lower, 16), count)

    def piece_rows(half, owner):
        return sub_rows(half, (2 + owner) * piece, piece)

    def half_rows(half, chunk):
        return pl.ds(pl.multiple_of(half * rows + chunk * unit, 16), unit)

    for at, other in enumerate((pd, px, py)):
        go(remote(wt.at[p], wt.at[p], s_fwd.at[at], r_fwd.at[at], other, t))
    mine = xc.at[p, piece_rows(k, z)]
    go(remote(mine, mine, s_fwd.at[3], r_fwd.at[3], pd, t))
    for chunk in range(CHUNKS):
        for at, other in enumerate((px, py)):
            sem = 4 + 2 * chunk + at
            mine = xc.at[p, half_rows(k, chunk)]
            go(remote(mine, mine, s_fwd.at[sem], r_fwd.at[sem], other, t))

    def arrived(ref, send, recv):
        remote(ref, ref, send, recv, p, mate).wait_recv()

    mine = xc.at[pd, piece_rows(k, z)]
    arrived(mine, s_fwd.at[3], r_fwd.at[3])
    for step in range(1, nz):
        go(remote(mine, mine, s_z.at[step], r_z.at[step], p, (t + 2 * step) % n_tp))
    go(remote(mine, mine, s_pair.at[0], r_pair.at[0], p, mate))
    for copy in local[4:]:
        copy.wait()
    arrived(wt.at[pd], s_fwd.at[0], r_fwd.at[0])
    arrived(wt.at[px], s_fwd.at[1], r_fwd.at[1])
    arrived(wt.at[py], s_fwd.at[2], r_fwd.at[2])

    nt = (((1,), (1,)), ((), ()))
    tn = (((0,), (0,)), ((), ()))

    def weights_of(b):
        at_expert = lax.broadcasted_iota(jnp.int32, wt.shape[1:], 0) == p
        row = jnp.sum(jnp.where(at_expert, wt[b], 0.0), axis=0, keepdims=True)
        return jnp.broadcast_to(row, (128, LANES)).T[:, 0:1]

    def compute(parts):
        count = sum(size for _, _, size in parts)

        def load(ref, shift, cols):
            got = [ref[b, pl.ds(shift + lower, size), cols] for b, lower, size in parts]
            return got[0] if len(got) == 1 else jnp.concatenate(got, axis=0)

        def store(ref, cols, value):
            done = 0
            for b, lower, size in parts:
                ref[b, pl.ds(lower, size), cols] = value[done:done + size]
                done += size

        every = slice(None)
        weight = [weights_of(b)[lower:lower + size] for b, lower, size in parts]
        weight = weight[0] if len(weight) == 1 else jnp.concatenate(weight, axis=0)
        tile = min(hidden_units, 256)
        route = jnp.zeros((count, 1), F32)
        for at in range(hidden_units // tile):
            cols = pl.ds(at * tile, tile)
            x = load(xc, 0, every)
            gate = jnp.dot(x, wg[:, cols], preferred_element_type=F32)
            up = jnp.dot(x, wu[:, cols], preferred_element_type=F32)
            back = lax.dot_general(load(xc, rows, every), wd[cols, :], nt, preferred_element_type=F32)
            sig = jax.nn.sigmoid(gate)
            active = gate * sig
            hidden = (active * up).astype(BF16)
            store(hid, cols, hidden)
            route = route + jnp.sum(hidden.astype(F32) * back, axis=1, keepdims=True)
            scaled = weight * back
            store(da, cols, (scaled * up * sig * (1.0 + gate * (1.0 - sig))).astype(BF16))
            store(db, cols, (scaled * active).astype(BF16))
        store(rcol, every, jnp.broadcast_to(route, (count, 128)))
        for at in range(nz):
            cols = pl.ds(2 * at * shard, 2 * shard)
            part = lax.dot_general(load(da, 0, every), wg[cols, :], nt, preferred_element_type=F32)
            part = part + lax.dot_general(load(db, 0, every), wu[cols, :], nt, preferred_element_type=F32)
            part, done = part.astype(BF16), 0
            for b, lower, size in parts:
                for core in range(2):
                    rp[core, at, b, pl.ds(lower, size), :] = part[done:done + size, core * shard:(core + 1) * shard]
                done += size
        for b, lower, size in parts:
            for chunk in range(lower // unit, (lower + size) // unit):
                span = pl.ds(chunk * unit, unit)
                sem = CHUNKS * orders[id(b)] + chunk
                go(remote(rp.at[1 - k, :, b, span], pr.at[:, b, span], s_rp.at[sem], r_rp.at[sem], p, mate))
        store(sc, every, (weight * load(xc, rows, every).astype(F32)).astype(BF16))

    orders = {id(p): 0, id(px): 1, id(py): 2, id(pd): 3}
    def add_pair(b, chunk):
        span = pl.ds(chunk * unit, unit)
        sem = CHUNKS * orders[id(b)] + chunk
        arrived(pr.at[:, b, span], s_rp.at[sem], r_rp.at[sem])
        for at in range(nz):
            rp[k, at, b, span, :] = (rp[k, at, b, span, :].astype(F32) + pr[at, b, span, :].astype(F32)).astype(BF16)

    def xy_sem(at, kind, chunk):
        return (kind * nz + at) * CHUNKS + chunk

    def first(at, b, kind, other, chunk):
        span = pl.ds(chunk * unit, unit)
        sem = xy_sem(at, kind, chunk)
        go(remote(rp.at[k, at, b, span], r1.at[at, kind, span], s_xy.at[sem], r_xy.at[sem], other, t))

    def first_near(chunk):
        add_pair(px, chunk)
        add_pair(py, chunk)
        for at in range(hz):
            first(at, px, 0, px, chunk)
            first(hz + at, py, 0, py, chunk)

    compute([(p, 0, rows)])
    for chunk in range(CHUNKS):
        for at, other in enumerate((px, py)):
            mine = xc.at[other, half_rows(k, chunk)]
            sem = 4 + 2 * chunk + at
            arrived(mine, s_fwd.at[sem], r_fwd.at[sem])
            go(remote(mine, mine, s_pair.at[sem], r_pair.at[sem], p, mate))
            if chunk == 0:
                passed = xc.at[other, sub_rows(k, at * piece, piece)]
                sem = 4 + 2 * CHUNKS + at
                go(remote(passed, passed, s_fwd.at[sem], r_fwd.at[sem], py if at == 0 else px, t))
        if chunk == CHUNKS - 1:
            for step in range(1, nz):
                mine = xc.at[pd, piece_rows(k, (z - step + nz) % nz)]
                arrived(mine, s_z.at[step], r_z.at[step])
                go(remote(mine, mine, s_pair.at[step], r_pair.at[step], p, mate))
        for at, other in enumerate((px, py)):
            sem = 4 + 2 * chunk + at
            arrived(xc.at[other, half_rows(1 - k, chunk)], s_pair.at[sem], r_pair.at[sem])
        compute([(px, chunk * unit, unit), (py, chunk * unit, unit)])
        if chunk == 0:
            add_pair(p, 0)
            add_pair(p, 1)
    for at in range(2):
        sem = 4 + 2 * CHUNKS + at
        passed = xc.at[pd, sub_rows(k, at * piece, piece)]
        arrived(passed, s_fwd.at[sem], r_fwd.at[sem])
        go(remote(passed, passed, s_pair.at[sem], r_pair.at[sem], p, mate))
    for chunk in range(CHUNKS):
        first_near(chunk)
    for at in range(2):
        sem = 4 + 2 * CHUNKS + at
        arrived(xc.at[pd, sub_rows(1 - k, at * piece, piece)], s_pair.at[sem], r_pair.at[sem])
    for step in range(nz):
        arrived(xc.at[pd, piece_rows(1 - k, (z - step + nz) % nz)], s_pair.at[step], r_pair.at[step])
    compute([(pd, 0, rows)])
    for chunk in range(CHUNKS):
        add_pair(pd, chunk)
        for at in range(hz):
            first(at, pd, 1, px, chunk)
            first(hz + at, pd, 1, py, chunk)

    for b in range(n_ep):
        rm[b:b + 1, :] = rcol[b].T[0:1, :]
    for step in range(1, n_tp):
        go(remote(rm, rr.at[step], s_rt.at[step], r_rt.at[step], p, (t + step) % n_tp))

    def wide(ref, lower, count, cols):
        got = ref[:, pl.ds(lower, count), cols]
        return got.reshape(n_ep * count, got.shape[2])

    def weight_grad(grads, out):
        @pl.loop(0, width // 256)
        def _(at):
            cols = pl.ds(pl.multiple_of(at * 256, 256), 256)
            out[cols, :] = lax.dot_general(
                wide(xc, 0, rows, cols), wide(grads, 0, rows, slice(None)), tn, preferred_element_type=F32
            ).astype(BF16)

    def second(at, b, other, chunk):
        span = pl.ds(chunk * unit, unit)
        sem = xy_sem(at, 1, chunk)
        arrived(r1.at[at, 1, span], s_xy.at[sem], r_xy.at[sem])
        rp[k, at, b, span, :] = (rp[k, at, b, span, :].astype(F32) + r1[at, 1, span, :].astype(F32)).astype(BF16)
        sem = xy_sem(at, 2, chunk)
        go(remote(rp.at[k, at, b, span], r2.at[at, span], s_xy.at[sem], r_xy.at[sem], other, t))

    def third(chunk):
        span = pl.ds(chunk * unit, unit)
        for at in range(nz):
            for kind, ref in ((0, r1.at[at, 0, span]), (2, r2.at[at, span])):
                sem = xy_sem(at, kind, chunk)
                arrived(ref, s_xy.at[sem], r_xy.at[sem])
            mine = rp[k, at, p, span, :].astype(F32) + r1[at, 0, span, :].astype(F32) + r2[at, span, :].astype(F32)
            rp[k, at, p, span, :] = mine.astype(BF16)
        for step in range(1, nz):
            sem = (1 + chunk) * nz + step
            go(remote(rp.at[k, (z + step) % nz, p, span], zr.at[step, span], s_z.at[sem], r_z.at[sem], p, (t + 2 * step) % n_tp))

    for chunk in range(CHUNKS):
        for at in range(hz):
            second(at, py, py, chunk)
            second(hz + at, px, px, chunk)

    total = rm[...]
    for step in range(1, n_tp):
        arrived(rr.at[step], s_rt.at[step], r_rt.at[step])
        total = total + rr[step]
    ra[...] = total
    for at, other in enumerate((px, py, pd)):
        go(remote(ra, rb.at[at], s_rt.at[n_tp + at], r_rt.at[n_tp + at], other, t))

    weight_grad(da, gg)
    third(0)
    weight_grad(db, gu)
    third(1)

    @pl.loop(0, hidden_units // 256)
    def _(at):
        units = pl.ds(pl.multiple_of(at * 256, 256), 256)
        left = wide(hid, 0, rows, units)

        @pl.loop(0, width // 512)
        def _(to):
            cols = pl.ds(pl.multiple_of(to * 512, 512), 512)
            gd[units, cols] = lax.dot_general(
                left, wide(sc, 0, rows, cols), tn, preferred_element_type=F32
            ).astype(BF16)

    index = lax.broadcasted_iota(jnp.int32, rm.shape, 0)
    result = jnp.zeros(rm.shape, F32)
    for at, other in enumerate((px, py, pd, p)):
        if at < 3:
            arrived(rb.at[at], s_rt.at[n_tp + at], r_rt.at[n_tp + at])
        got = rb[at] if at < 3 else ra[...]
        row = jnp.sum(jnp.where(index == p, got, 0.0), axis=0, keepdims=True)
        result = result + jnp.where(index == other, row, 0.0)
    for choice in range(routes_ref.shape[0]):
        hit = routes_ref[choice:choice + 1, :] == experts
        rt_ref[choice:choice + 1, :] = jnp.sum(jnp.where(hit, result[:, 0:rows], 0.0), axis=0, keepdims=True)

    total = rp[k, z, p].astype(F32)
    for step in range(1, nz):
        for chunk in range(CHUNKS):
            sem = (1 + chunk) * nz + step
            arrived(zr.at[step, pl.ds(chunk * unit, unit)], s_z.at[sem], r_z.at[sem])
        total = total + zr[step].astype(F32)
    gt_ref[...] = total.astype(BF16)
    for copy in sends:
        copy.wait_send()


def write_kernel(*refs):
    sem = refs[-1]
    copies = [pltpu.make_async_copy(refs[at], refs[5 + at], sem.at[at]) for at in range(5)]
    for copy in copies:
        copy.start()
    for copy in copies:
        copy.wait()


def fused(n_ep, n_tp, tokens, cotangent, routes, route_weight, gate_weight, up_weight, down_weight):
    rows, width = tokens.shape
    units = gate_weight.shape[2]
    nz = n_tp // 2
    shard = width // n_tp
    hbm, vmem = pl.BlockSpec(memory_space=pltpu.HBM), pl.BlockSpec(memory_space=pltpu.VMEM)
    dma = pltpu.SemaphoreType.DMA
    grad_tokens, by_choice, grad_gate, grad_up, grad_down = pl.pallas_call(
        functools.partial(step_kernel, n_ep, n_tp),
        out_shape=(
            jax.ShapeDtypeStruct((rows, shard), BF16),
            jax.ShapeDtypeStruct((routes.shape[1], rows), F32),
            jax.ShapeDtypeStruct((width, units), BF16),
            jax.ShapeDtypeStruct((width, units), BF16),
            jax.ShapeDtypeStruct((units, width), BF16),
        ),
        in_specs=[hbm] * 7,
        out_specs=(vmem,) * 5,
        scratch_shapes=[
            pltpu.VMEM((routes.shape[1], rows), jnp.int32),
            pltpu.VMEM((routes.shape[1], rows), F32),
            pltpu.VMEM((n_ep, 2 * rows, width), BF16),
            pltpu.VMEM((n_ep, 8, LANES), F32),
            pltpu.VMEM((width, units), BF16),
            pltpu.VMEM((width, units), BF16),
            pltpu.VMEM((units, width), BF16),
            pltpu.VMEM((n_ep, rows, units), BF16),
            pltpu.VMEM((n_ep, rows, units), BF16),
            pltpu.VMEM((n_ep, rows, units), BF16),
            pltpu.VMEM((n_ep, rows, width), BF16),
            pltpu.VMEM((2, nz, n_ep, rows, shard), BF16),
            pltpu.VMEM((nz, n_ep, rows, shard), BF16),
            pltpu.VMEM((nz, 2, rows, shard), BF16),
            pltpu.VMEM((nz, rows, shard), BF16),
            pltpu.VMEM((nz, rows, shard), BF16),
            pltpu.VMEM((n_ep, LANES, 128), F32),
            pltpu.VMEM((8, LANES), F32),
            pltpu.VMEM((n_tp, 8, LANES), F32),
            pltpu.VMEM((8, LANES), F32),
            pltpu.VMEM((3, 8, LANES), F32),
            dma((7,)),
            dma((6 + 2 * CHUNKS,)),
            dma((6 + 2 * CHUNKS,)),
            dma((6 + 2 * CHUNKS,)),
            dma((6 + 2 * CHUNKS,)),
            dma((n_ep * CHUNKS,)),
            dma((n_ep * CHUNKS,)),
            dma((3 * nz * CHUNKS,)),
            dma((3 * nz * CHUNKS,)),
            dma(((1 + CHUNKS) * nz,)),
            dma(((1 + CHUNKS) * nz,)),
            dma((n_tp + 3,)),
            dma((n_tp + 3,)),
        ],
        compiler_params=pltpu.CompilerParams(
            collective_id=0, has_side_effects=True, vmem_limit_bytes=VLIM * 1024 * 1024
        ),
    )(*(pltpu.with_memory_space_constraint(array, pltpu.HBM) for array in (
        tokens, cotangent, routes.T, route_weight.T, gate_weight[0], up_weight[0], down_weight[0]
    )))
    results = (grad_tokens, by_choice, grad_gate, grad_up, grad_down)
    grad_tokens, by_choice, grad_gate, grad_up, grad_down = pl.pallas_call(
        write_kernel,
        out_shape=tuple(jax.ShapeDtypeStruct(array.shape, array.dtype) for array in results),
        in_specs=[vmem] * 5,
        out_specs=(hbm,) * 5,
        scratch_shapes=[dma((5,))],
        compiler_params=pltpu.CompilerParams(vmem_limit_bytes=1024 * 1024),
    )(*results)
    grad_route = by_choice.T
    return grad_tokens, grad_route, grad_gate[None], grad_up[None], grad_down[None]


def body(mesh, *arrays):
    n_ep, n_tp = mesh.shape["ep"], mesh.shape["tp"]
    rows, width = arrays[0].shape
    experts, _, units = arrays[4].shape
    capacity = 2 * rows * arrays[2].shape[1] // (experts * n_ep)
    fits = (
        n_ep == 4 and experts == 1 and n_tp == 8 and capacity >= rows and rows <= LANES
        and width % (n_tp * 128) == 0 and width % 512 == 0 and units % 256 == 0
        and rows % (16 * (n_tp // 2 + 2)) == 0 and 2 * (rows // (n_tp // 2 + 2)) <= rows // CHUNKS and rows % (16 * CHUNKS) == 0
    )
    return fused(n_ep, n_tp, *arrays) if fits else shards(*arrays)


def solution(mesh):
    return jax.shard_map(
        functools.partial(body, mesh),
        mesh=mesh,
        in_specs=(
            P("ep", None),
            P("ep", None),
            P("ep", None),
            P("ep", None),
            P("ep", None, "tp"),
            P("ep", None, "tp"),
            P("ep", "tp", None),
        ),
        out_specs=(
            P("ep", "tp"),
            P("ep", None),
            P("ep", None, "tp"),
            P("ep", None, "tp"),
            P("ep", "tp", None),
        ),
        check_vma=False,
    )
```

```python
import functools

import jax
import jax.numpy as jnp
from jax import lax
from jax.experimental import pallas as pl
from jax.experimental.pallas import tpu as pltpu
from jax.sharding import PartitionSpec as P

F32, BF16 = jnp.float32, jnp.bfloat16
LANES = 256
CHUNKS = 3
PARTS = 4
VLIM = 40


def shards(tokens, cotangent, routes, route_weight, gate_weight, up_weight, down_weight):
    rows, model_width = tokens.shape
    top = routes.shape[1]
    local_experts = gate_weight.shape[0]
    experts_all = local_experts * lax.axis_size("ep")
    capacity = 2 * rows * top // experts_all
    shard_width = model_width // lax.axis_size("tp")
    flat_routes = routes.reshape(-1)
    expert_ids = jnp.arange(experts_all, dtype=jnp.int32)
    onehot_table = (flat_routes[:, None] == expert_ids[None, :]).astype(jnp.int32)
    earlier = jnp.cumsum(onehot_table, axis=0) - onehot_table
    order_in = jnp.sum(earlier * onehot_table, axis=1)
    slot_index = flat_routes * capacity + order_in
    entries = jnp.arange(rows * top, dtype=jnp.int32) + 1
    slot_table = jnp.zeros((experts_all * capacity,), jnp.int32).at[slot_index].set(entries)
    filled = slot_table > 0
    entry = jnp.maximum(slot_table - 1, 0)
    source_row = entry // top
    zero_value = jnp.zeros((), jnp.bfloat16)
    token_buf = jnp.where(filled[:, None], tokens[source_row], zero_value).reshape(
        experts_all, capacity, model_width
    )
    cot_buf = jnp.where(filled[:, None], cotangent[source_row], zero_value).reshape(
        experts_all, capacity, model_width
    )
    weight_buf = (
        jnp.where(filled, route_weight.reshape(-1)[entry], 0.0)
        .astype(jnp.bfloat16)
        .reshape(experts_all, capacity)
    )
    start = lax.axis_index("tp") * shard_width
    token_part = lax.dynamic_slice_in_dim(token_buf, start, shard_width, 2)
    cot_part = lax.dynamic_slice_in_dim(cot_buf, start, shard_width, 2)
    token_part, cot_part, arrived_weight = (
        lax.all_to_all(token_part, "ep", split_axis=0, concat_axis=1, tiled=True),
        lax.all_to_all(cot_part, "ep", split_axis=0, concat_axis=1, tiled=True),
        lax.all_to_all(weight_buf, "ep", split_axis=0, concat_axis=1, tiled=True),
    )
    arrived_tokens, arrived_cot = (
        lax.all_gather(token_part, "tp", axis=2, tiled=True),
        lax.all_gather(cot_part, "tp", axis=2, tiled=True),
    )
    gate_pre = jnp.einsum(
        "erd,edf->erf", arrived_tokens, gate_weight, preferred_element_type=jnp.float32
    )
    up_pre = jnp.einsum(
        "erd,edf->erf", arrived_tokens, up_weight, preferred_element_type=jnp.float32
    )
    sig = jax.nn.sigmoid(gate_pre)
    active = gate_pre * sig
    hidden = (active * up_pre).astype(jnp.bfloat16)
    back_raw = jnp.einsum(
        "erd,efd->erf", arrived_cot, down_weight, preferred_element_type=jnp.float32
    )
    route_part = jnp.sum(hidden.astype(jnp.float32) * back_raw, axis=2)
    slot_weight = arrived_weight.astype(jnp.float32)
    scaled_back = slot_weight[:, :, None] * back_raw
    grad_gate_pre = (scaled_back * up_pre * sig * (1.0 + gate_pre * (1.0 - sig))).astype(
        jnp.bfloat16
    )
    grad_up_pre = (scaled_back * active).astype(jnp.bfloat16)
    scaled_cot = (slot_weight[:, :, None] * arrived_cot).astype(jnp.bfloat16)
    grad_gate = jnp.einsum(
        "erd,erf->edf", arrived_tokens, grad_gate_pre, preferred_element_type=jnp.float32
    ).astype(jnp.bfloat16)
    grad_up = jnp.einsum(
        "erd,erf->edf", arrived_tokens, grad_up_pre, preferred_element_type=jnp.float32
    ).astype(jnp.bfloat16)
    grad_down = jnp.einsum(
        "erf,erd->efd", hidden, scaled_cot, preferred_element_type=jnp.float32
    ).astype(jnp.bfloat16)
    row_part = jnp.einsum(
        "erf,edf->erd", grad_gate_pre, gate_weight, preferred_element_type=jnp.float32
    )
    row_part = row_part + jnp.einsum(
        "erf,edf->erd", grad_up_pre, up_weight, preferred_element_type=jnp.float32
    )
    row_summed = lax.psum_scatter(
        row_part.astype(jnp.bfloat16), "tp", scatter_dimension=2, tiled=True
    )
    returned = lax.all_to_all(row_summed, "ep", split_axis=1, concat_axis=0, tiled=True)
    route_total = lax.psum(route_part, "tp")
    route_back = lax.all_to_all(route_total, "ep", split_axis=1, concat_axis=0, tiled=True)
    per_entry = returned.reshape(experts_all * capacity, shard_width)[slot_index]
    grad_tokens = jnp.sum(
        per_entry.astype(jnp.float32).reshape(rows, top, shard_width), axis=1
    ).astype(jnp.bfloat16)
    grad_route = route_back.reshape(-1)[slot_index].reshape(rows, top)
    return (grad_tokens, grad_route, grad_gate, grad_up, grad_down)


def step_kernel(
    n_ep, n_tp,
    x_hbm, c_hbm, routes_hbm, weight_hbm, wg_hbm, wu_hbm, wd_hbm,
    gt_ref, rt_ref, gg, gu, gd,
    routes_ref, weight_ref, wgt, wut, wdt, xc, wt, wg, wu, wd, hid, da, db, sc, rp, pr, r1, r2, zr, rcol, rm, rr, ra, rb,
    zq, rq, s_zf, r_zf, s_rq, r_rq, lsem, s_fwd, r_fwd, s_pair, r_pair, s_rp, r_rp, s_xy, r_xy, s_z, r_z, s_rt, r_rt,
):
    nz = n_tp // 2
    hz = nz // 2
    rows, width = x_hbm.shape
    hidden_units = wg.shape[1]
    shard = width // n_tp
    piece = rows // (nz + 2)
    cuts = (0, 2 * piece, rows - piece, rows)
    middle = 2 * piece + (rows - 3 * piece) // 32 * 16
    ends = (0, 2 * piece, middle, rows - piece, rows)
    p, t = lax.axis_index("ep"), lax.axis_index("tp")
    k, z = t % 2, t // 2
    px, py, pd = p + 1 - 2 * (p % 2), p + 2 - 4 * (p // 2), 3 - p
    mate = t + 1 - 2 * k

    def remote(src, dst, send, recv, ep, tp):
        return pltpu.make_async_remote_copy(
            src_ref=src, dst_ref=dst, send_sem=send, recv_sem=recv,
            device_id={"ep": ep, "tp": tp}, device_id_type=pl.DeviceIdType.MESH,
        )

    local = [
        pltpu.make_async_copy(x_hbm, xc.at[p, pl.ds(0, rows)], lsem.at[0]),
        pltpu.make_async_copy(c_hbm, xc.at[p, pl.ds(rows, rows)], lsem.at[1]),
        pltpu.make_async_copy(routes_hbm, routes_ref, lsem.at[5]),
        pltpu.make_async_copy(weight_hbm, weight_ref, lsem.at[6]),
        pltpu.make_async_copy(wg_hbm, wg, lsem.at[2]),
        pltpu.make_async_copy(wu_hbm, wu, lsem.at[3]),
        pltpu.make_async_copy(wd_hbm, wd, lsem.at[4]),
    ]
    for copy in local:
        copy.start()
    barrier = pltpu.get_barrier_semaphore()
    for other in (px, py, pd):
        pl.semaphore_signal(barrier, inc=1, device_id={"ep": other, "tp": t}, device_id_type=pl.DeviceIdType.MESH)
    for step in range(1, n_tp):
        pl.semaphore_signal(barrier, inc=1, device_id={"ep": p, "tp": (t + step) % n_tp}, device_id_type=pl.DeviceIdType.MESH)
    for copy in local[2:4]:
        copy.wait()
    experts = lax.broadcasted_iota(jnp.int32, (8, rows), 0)
    mixed = jnp.zeros((8, rows), F32)
    for choice in range(routes_ref.shape[0]):
        hit = routes_ref[choice:choice + 1, :] == experts
        mixed = mixed + jnp.where(hit, weight_ref[choice:choice + 1, :], 0.0)
    wt[p] = jnp.zeros(wt.shape[1:], F32)
    wt[p, :, 0:rows] = mixed.astype(BF16).astype(F32)
    pl.semaphore_wait(barrier, n_ep - 1 + n_tp - 1)
    for copy in local[:2]:
        copy.wait()

    sends = []

    def go(copy):
        copy.start()
        sends.append(copy)

    def sub_rows(half, lower, count):
        return pl.ds(pl.multiple_of(half * rows + lower, 16), count)

    def piece_rows(half, owner):
        return sub_rows(half, (2 + owner) * piece, piece)

    def half_rows(half, part):
        return sub_rows(half, ends[part], ends[part + 1] - ends[part])

    def span_of(chunk):
        return pl.ds(cuts[chunk], cuts[chunk + 1] - cuts[chunk])

    for at, other in enumerate((pd, px, py)):
        go(remote(wt.at[p], wt.at[p], s_fwd.at[at], r_fwd.at[at], other, t))
    mine = xc.at[p, piece_rows(k, z)]
    go(remote(mine, mine, s_fwd.at[3], r_fwd.at[3], pd, t))

    def send_near(part):
        for at, other in enumerate((px, py)):
            sem = 4 + 2 * part + at
            mine = xc.at[p, half_rows(k, part)]
            go(remote(mine, mine, s_fwd.at[sem], r_fwd.at[sem], other, t))

    send_near(0)
    send_near(1)

    def arrived(ref, send, recv):
        remote(ref, ref, send, recv, p, mate).wait_recv()

    for copy in local[4:]:
        copy.wait()
    tn = (((0,), (0,)), ((), ()))

    def weights_of(b):
        at_expert = lax.broadcasted_iota(jnp.int32, wt.shape[1:], 0) == p
        row = jnp.sum(jnp.where(at_expert, wt[b], 0.0), axis=0, keepdims=True)
        return jnp.broadcast_to(row, (128, LANES)).T[:, 0:1]

    def compute(parts):
        count = sum(size for _, _, size in parts)

        def load(ref, shift, cols):
            got = [ref[b, pl.ds(shift + lower, size), cols] for b, lower, size in parts]
            return got[0] if len(got) == 1 else jnp.concatenate(got, axis=0)

        def store(ref, cols, value):
            done = 0
            for b, lower, size in parts:
                ref[b, pl.ds(lower, size), cols] = value[done:done + size]
                done += size

        every = slice(None)
        weight = [weights_of(b)[lower:lower + size] for b, lower, size in parts]
        weight = weight[0] if len(weight) == 1 else jnp.concatenate(weight, axis=0)
        tile = min(hidden_units, 256)
        route = jnp.zeros((count, 1), F32)
        for at in range(hidden_units // tile):
            cols = pl.ds(at * tile, tile)
            x = load(xc, 0, every)
            gate = jnp.dot(x, wg[:, cols], preferred_element_type=F32)
            up = jnp.dot(x, wu[:, cols], preferred_element_type=F32)
            back = jnp.dot(load(xc, rows, every), wdt[:, cols], preferred_element_type=F32)
            sig = jax.nn.sigmoid(gate)
            active = gate * sig
            hidden = (active * up).astype(BF16)
            store(hid, cols, hidden)
            route = route + jnp.sum(hidden.astype(F32) * back, axis=1, keepdims=True)
            scaled = weight * back
            store(da, cols, (scaled * up * sig * (1.0 + gate * (1.0 - sig))).astype(BF16))
            store(db, cols, (scaled * active).astype(BF16))
        store(rcol, every, jnp.broadcast_to(route, (count, 128)))
        for at in range(nz):
            cols = pl.ds(2 * at * shard, 2 * shard)
            part = jnp.dot(load(da, 0, every), wgt[:, cols], preferred_element_type=F32)
            part = part + jnp.dot(load(db, 0, every), wut[:, cols], preferred_element_type=F32)
            part, done = part.astype(BF16), 0
            for b, lower, size in parts:
                for core in range(2):
                    rp[core, at, b, pl.ds(lower, size), :] = part[done:done + size, core * shard:(core + 1) * shard]
                done += size
        for b, lower, size in parts:
            for chunk in range(CHUNKS):
                if not lower <= cuts[chunk] < lower + size:
                    continue
                span = span_of(chunk)
                sem = CHUNKS * orders[id(b)] + chunk
                go(remote(rp.at[1 - k, :, b, span], pr.at[:, b, span], s_rp.at[sem], r_rp.at[sem], p, mate))
        store(sc, every, (weight * load(xc, rows, every).astype(F32)).astype(BF16))

    orders = {id(p): 0, id(px): 1, id(py): 2, id(pd): 3}
    def add_pair(b, chunk):
        span = span_of(chunk)
        sem = CHUNKS * orders[id(b)] + chunk
        arrived(pr.at[:, b, span], s_rp.at[sem], r_rp.at[sem])
        for at in range(nz):
            rp[k, at, b, span, :] = (rp[k, at, b, span, :].astype(F32) + pr[at, b, span, :].astype(F32)).astype(BF16)

    def z_first(b):
        add_pair(b, 0)
        for step in range(1, nz):
            sem = orders[id(b)] * nz + step
            go(remote(
                rp.at[k, (z + step) % nz, b, span_of(0)], zq.at[step, orders[id(b)]],
                s_zf.at[sem], r_zf.at[sem], p, (t + 2 * step) % n_tp,
            ))

    def z_sum(b):
        at, span = orders[id(b)], span_of(0)
        total = rp[k, z, b, span, :].astype(F32)
        for step in range(1, nz):
            sem = at * nz + step
            arrived(zq.at[step, at], s_zf.at[sem], r_zf.at[sem])
            total = total + zq[step, at].astype(F32)
        rp[k, z, b, span, :] = total.astype(BF16)
        if at:
            go(remote(rp.at[k, z, b, span], rq.at[at - 1], s_rq.at[at - 1], r_rq.at[at - 1], b, t))

    def xy_sem(at, kind, chunk):
        return (kind * nz + at) * CHUNKS + chunk

    def first(at, b, kind, other, chunk):
        span = span_of(chunk)
        sem = xy_sem(at, kind, chunk)
        go(remote(rp.at[k, at, b, span], r1.at[at, kind, span], s_xy.at[sem], r_xy.at[sem], other, t))

    def first_near(chunk):
        add_pair(px, chunk)
        add_pair(py, chunk)
        for at in range(hz):
            first(at, px, 0, px, chunk)
            first(hz + at, py, 0, py, chunk)

    def first_pd(chunks):
        for chunk in chunks:
            add_pair(pd, chunk)
            for at in range(hz):
                first(at, pd, 1, px, chunk)
                first(hz + at, pd, 1, py, chunk)

    def take_near(part):
        for at, other in enumerate((px, py)):
            mine = xc.at[other, half_rows(k, part)]
            sem = 4 + 2 * part + at
            arrived(mine, s_fwd.at[sem], r_fwd.at[sem])
            go(remote(mine, mine, s_pair.at[sem], r_pair.at[sem], p, mate))

    def wait_near(part):
        for at, other in enumerate((px, py)):
            sem = 4 + 2 * part + at
            arrived(xc.at[other, half_rows(1 - k, part)], s_pair.at[sem], r_pair.at[sem])

    def compute_near(chunk):
        lower, size = cuts[chunk], cuts[chunk + 1] - cuts[chunk]
        compute([(px, lower, size), (py, lower, size)])

    for at in range(width // 512):
        for to in range(hidden_units // 256):
            a, b = pl.ds(at * 512, 512), pl.ds(to * 256, 256)
            wgt[b, a] = wg[a, b].T
            wut[b, a] = wu[a, b].T
            wdt[a, b] = wd[b, a].T
    compute([(p, 0, rows)])
    mine = xc.at[pd, piece_rows(k, z)]
    arrived(mine, s_fwd.at[3], r_fwd.at[3])
    for step in range(1, nz):
        go(remote(mine, mine, s_z.at[step], r_z.at[step], p, (t + 2 * step) % n_tp))
    go(remote(mine, mine, s_pair.at[0], r_pair.at[0], p, mate))
    take_near(0)
    for at, other in enumerate((px, py)):
        passed = xc.at[other, sub_rows(k, at * piece, piece)]
        sem = 4 + 2 * PARTS + at
        go(remote(passed, passed, s_fwd.at[sem], r_fwd.at[sem], py if at == 0 else px, t))
    send_near(2)
    send_near(3)
    for chunk in range(1, CHUNKS):
        add_pair(p, chunk)
    arrived(wt.at[pd], s_fwd.at[0], r_fwd.at[0])
    arrived(wt.at[px], s_fwd.at[1], r_fwd.at[1])
    arrived(wt.at[py], s_fwd.at[2], r_fwd.at[2])
    wait_near(0)
    compute_near(0)
    take_near(1)
    for step in range(1, nz):
        mine = xc.at[pd, piece_rows(k, (z - step + nz) % nz)]
        arrived(mine, s_z.at[step], r_z.at[step])
        go(remote(mine, mine, s_pair.at[step], r_pair.at[step], p, mate))
    z_first(p)
    z_first(px)
    z_first(py)
    for at in range(2):
        sem = 4 + 2 * PARTS + at
        passed = xc.at[pd, sub_rows(k, at * piece, piece)]
        arrived(passed, s_fwd.at[sem], r_fwd.at[sem])
        go(remote(passed, passed, s_pair.at[sem], r_pair.at[sem], p, mate))
    for at in range(2):
        sem = 4 + 2 * PARTS + at
        arrived(xc.at[pd, sub_rows(1 - k, at * piece, piece)], s_pair.at[sem], r_pair.at[sem])
    for step in range(nz):
        arrived(xc.at[pd, piece_rows(1 - k, (z - step + nz) % nz)], s_pair.at[step], r_pair.at[step])
    compute([(pd, 0, rows)])
    take_near(2)
    first_pd(range(1, CHUNKS))
    z_first(pd)
    z_sum(p)
    wait_near(1)
    wait_near(2)
    compute_near(1)
    take_near(3)
    z_sum(px)
    z_sum(py)
    first_near(1)
    wait_near(3)
    compute_near(2)

    def wide(ref, lower, count, cols):
        got = ref[:, pl.ds(lower, count), cols]
        return got.reshape(n_ep * count, got.shape[2])

    def up_grads(*slices):
        for at in slices:
            cols = pl.ds(at * (width // 8), width // 8)
            left = wide(xc, 0, rows, cols)
            for grads, out in ((da, gg), (db, gu)):
                out[cols, :] = lax.dot_general(
                    left, wide(grads, 0, rows, slice(None)), tn, preferred_element_type=F32
                ).astype(BF16)

    def down_grads(*slices):
        for at in slices:
            cols = pl.ds(at * (width // 4), width // 4)
            gd[:, cols] = lax.dot_general(
                wide(hid, 0, rows, slice(None)), wide(sc, 0, rows, cols), tn, preferred_element_type=F32
            ).astype(BF16)

    def second(at, b, other, chunk):
        span = span_of(chunk)
        sem = xy_sem(at, 1, chunk)
        arrived(r1.at[at, 1, span], s_xy.at[sem], r_xy.at[sem])
        rp[k, at, b, span, :] = (rp[k, at, b, span, :].astype(F32) + r1[at, 1, span, :].astype(F32)).astype(BF16)
        sem = xy_sem(at, 2, chunk)
        go(remote(rp.at[k, at, b, span], r2.at[at, span], s_xy.at[sem], r_xy.at[sem], other, t))

    def third(chunk):
        span = span_of(chunk)
        for at in range(nz):
            for kind, ref in ((0, r1.at[at, 0, span]), (2, r2.at[at, span])):
                sem = xy_sem(at, kind, chunk)
                arrived(ref, s_xy.at[sem], r_xy.at[sem])
            mine = rp[k, at, p, span, :].astype(F32) + r1[at, 0, span, :].astype(F32) + r2[at, span, :].astype(F32)
            rp[k, at, p, span, :] = mine.astype(BF16)
        for step in range(1, nz):
            sem = (1 + chunk) * nz + step
            go(remote(rp.at[k, (z + step) % nz, p, span], zr.at[step, span], s_z.at[sem], r_z.at[sem], p, (t + 2 * step) % n_tp))

    def second_both(chunk):
        for at in range(hz):
            second(at, py, py, chunk)
            second(hz + at, px, px, chunk)

    def send_route():
        for b in range(n_ep):
            rm[b:b + 1, :] = rcol[b].T[0:1, :]
        for step in range(1, n_tp):
            go(remote(rm, rr.at[step], s_rt.at[step], r_rt.at[step], p, (t + step) % n_tp))

    def return_route():
        total = rm[...]
        for step in range(1, n_tp):
            arrived(rr.at[step], s_rt.at[step], r_rt.at[step])
            total = total + rr[step]
        ra[...] = total
        for at, other in enumerate((px, py, pd)):
            go(remote(ra, rb.at[at], s_rt.at[n_tp + at], r_rt.at[n_tp + at], other, t))

    second_both(1)
    up_grads(0)
    first_near(2)
    second_both(2)
    z_sum(pd)
    send_route()
    up_grads(1, 2)
    third(1)
    up_grads(3, 4)
    return_route()
    third(2)
    up_grads(5, 6, 7)
    down_grads(0, 1, 2, 3)

    index = lax.broadcasted_iota(jnp.int32, rm.shape, 0)
    result = jnp.zeros(rm.shape, F32)
    for at, other in enumerate((px, py, pd, p)):
        if at < 3:
            arrived(rb.at[at], s_rt.at[n_tp + at], r_rt.at[n_tp + at])
        got = rb[at] if at < 3 else ra[...]
        row = jnp.sum(jnp.where(index == p, got, 0.0), axis=0, keepdims=True)
        result = result + jnp.where(index == other, row, 0.0)
    for choice in range(routes_ref.shape[0]):
        hit = routes_ref[choice:choice + 1, :] == experts
        rt_ref[choice:choice + 1, :] = jnp.sum(jnp.where(hit, result[:, 0:rows], 0.0), axis=0, keepdims=True)

    total = rp[k, z, p, span_of(0), :].astype(F32)
    for at in range(3):
        arrived(rq.at[at], s_rq.at[at], r_rq.at[at])
        total = total + rq[at].astype(F32)
    gt_ref[span_of(0), :] = total.astype(BF16)
    for chunk in range(1, CHUNKS):
        span = span_of(chunk)
        total = rp[k, z, p, span, :].astype(F32)
        for step in range(1, nz):
            sem = (1 + chunk) * nz + step
            arrived(zr.at[step, span], s_z.at[sem], r_z.at[sem])
            total = total + zr[step, span, :].astype(F32)
        gt_ref[span, :] = total.astype(BF16)
    for copy in sends:
        copy.wait_send()


def write_kernel(*refs):
    sem = refs[-1]
    copies = [pltpu.make_async_copy(refs[at], refs[5 + at], sem.at[at]) for at in range(5)]
    for copy in copies:
        copy.start()
    for copy in copies:
        copy.wait()


def fused(n_ep, n_tp, tokens, cotangent, routes, route_weight, gate_weight, up_weight, down_weight):
    rows, width = tokens.shape
    units = gate_weight.shape[2]
    nz = n_tp // 2
    shard = width // n_tp
    hbm, vmem = pl.BlockSpec(memory_space=pltpu.HBM), pl.BlockSpec(memory_space=pltpu.VMEM)
    dma = pltpu.SemaphoreType.DMA
    grad_tokens, by_choice, grad_gate, grad_up, grad_down = pl.pallas_call(
        functools.partial(step_kernel, n_ep, n_tp),
        out_shape=(
            jax.ShapeDtypeStruct((rows, shard), BF16),
            jax.ShapeDtypeStruct((routes.shape[1], rows), F32),
            jax.ShapeDtypeStruct((width, units), BF16),
            jax.ShapeDtypeStruct((width, units), BF16),
            jax.ShapeDtypeStruct((units, width), BF16),
        ),
        in_specs=[hbm] * 7,
        out_specs=(vmem,) * 5,
        scratch_shapes=[
            pltpu.VMEM((routes.shape[1], rows), jnp.int32),
            pltpu.VMEM((routes.shape[1], rows), F32),
            pltpu.VMEM((units, width), BF16),
            pltpu.VMEM((units, width), BF16),
            pltpu.VMEM((width, units), BF16),
            pltpu.VMEM((n_ep, 2 * rows, width), BF16),
            pltpu.VMEM((n_ep, 8, LANES), F32),
            pltpu.VMEM((width, units), BF16),
            pltpu.VMEM((width, units), BF16),
            pltpu.VMEM((units, width), BF16),
            pltpu.VMEM((n_ep, rows, units), BF16),
            pltpu.VMEM((n_ep, rows, units), BF16),
            pltpu.VMEM((n_ep, rows, units), BF16),
            pltpu.VMEM((n_ep, rows, width), BF16),
            pltpu.VMEM((2, nz, n_ep, rows, shard), BF16),
            pltpu.VMEM((nz, n_ep, rows, shard), BF16),
            pltpu.VMEM((nz, 2, rows, shard), BF16),
            pltpu.VMEM((nz, rows, shard), BF16),
            pltpu.VMEM((nz, rows, shard), BF16),
            pltpu.VMEM((n_ep, LANES, 128), F32),
            pltpu.VMEM((8, LANES), F32),
            pltpu.VMEM((n_tp, 8, LANES), F32),
            pltpu.VMEM((8, LANES), F32),
            pltpu.VMEM((3, 8, LANES), F32),
            pltpu.VMEM((nz, n_ep, 2 * (rows // (nz + 2)), shard), BF16),
            pltpu.VMEM((3, 2 * (rows // (nz + 2)), shard), BF16),
            dma((n_ep * nz,)),
            dma((n_ep * nz,)),
            dma((3,)),
            dma((3,)),
            dma((7,)),
            dma((6 + 2 * PARTS,)),
            dma((6 + 2 * PARTS,)),
            dma((6 + 2 * PARTS,)),
            dma((6 + 2 * PARTS,)),
            dma((n_ep * CHUNKS,)),
            dma((n_ep * CHUNKS,)),
            dma((3 * nz * CHUNKS,)),
            dma((3 * nz * CHUNKS,)),
            dma(((1 + CHUNKS) * nz,)),
            dma(((1 + CHUNKS) * nz,)),
            dma((n_tp + 3,)),
            dma((n_tp + 3,)),
        ],
        compiler_params=pltpu.CompilerParams(
            collective_id=0, has_side_effects=True, vmem_limit_bytes=VLIM * 1024 * 1024
        ),
    )(*(pltpu.with_memory_space_constraint(array, pltpu.HBM) for array in (
        tokens, cotangent, routes.T, route_weight.T, gate_weight[0], up_weight[0], down_weight[0]
    )))
    results = (grad_tokens, by_choice, grad_gate, grad_up, grad_down)
    grad_tokens, by_choice, grad_gate, grad_up, grad_down = pl.pallas_call(
        write_kernel,
        out_shape=tuple(jax.ShapeDtypeStruct(array.shape, array.dtype) for array in results),
        in_specs=[vmem] * 5,
        out_specs=(hbm,) * 5,
        scratch_shapes=[dma((5,))],
        compiler_params=pltpu.CompilerParams(vmem_limit_bytes=1024 * 1024),
    )(*results)
    grad_route = by_choice.T
    return grad_tokens, grad_route, grad_gate[None], grad_up[None], grad_down[None]


def body(mesh, *arrays):
    n_ep, n_tp = mesh.shape["ep"], mesh.shape["tp"]
    rows, width = arrays[0].shape
    experts, _, units = arrays[4].shape
    capacity = 2 * rows * arrays[2].shape[1] // (experts * n_ep)
    fits = (
        n_ep == 4 and experts == 1 and n_tp == 8 and capacity >= rows and rows <= LANES
        and width % (n_tp * 128) == 0 and width % 512 == 0 and units % 256 == 0
        and units >= 512 and width % 1024 == 0 and rows % (16 * (n_tp // 2 + 2)) == 0
    )
    return fused(n_ep, n_tp, *arrays) if fits else shards(*arrays)


def solution(mesh):
    return jax.shard_map(
        functools.partial(body, mesh),
        mesh=mesh,
        in_specs=(
            P("ep", None),
            P("ep", None),
            P("ep", None),
            P("ep", None),
            P("ep", None, "tp"),
            P("ep", None, "tp"),
            P("ep", "tp", None),
        ),
        out_specs=(
            P("ep", "tp"),
            P("ep", None),
            P("ep", None, "tp"),
            P("ep", None, "tp"),
            P("ep", "tp", None),
        ),
        check_vma=False,
    )
```

```python
import functools

import jax
import jax.numpy as jnp
from jax import lax
from jax.experimental import pallas as pl
from jax.experimental.pallas import tpu as pltpu
from jax.sharding import PartitionSpec as P

F32, BF16 = jnp.float32, jnp.bfloat16
LANES = 256
CHUNKS = 4
PARTS = 4
VLIM = 40


def shards(tokens, cotangent, routes, route_weight, gate_weight, up_weight, down_weight):
    rows, model_width = tokens.shape
    top = routes.shape[1]
    local_experts = gate_weight.shape[0]
    experts_all = local_experts * lax.axis_size("ep")
    capacity = 2 * rows * top // experts_all
    shard_width = model_width // lax.axis_size("tp")
    flat_routes = routes.reshape(-1)
    expert_ids = jnp.arange(experts_all, dtype=jnp.int32)
    onehot_table = (flat_routes[:, None] == expert_ids[None, :]).astype(jnp.int32)
    earlier = jnp.cumsum(onehot_table, axis=0) - onehot_table
    order_in = jnp.sum(earlier * onehot_table, axis=1)
    slot_index = flat_routes * capacity + order_in
    entries = jnp.arange(rows * top, dtype=jnp.int32) + 1
    slot_table = jnp.zeros((experts_all * capacity,), jnp.int32).at[slot_index].set(entries)
    filled = slot_table > 0
    entry = jnp.maximum(slot_table - 1, 0)
    source_row = entry // top
    zero_value = jnp.zeros((), jnp.bfloat16)
    token_buf = jnp.where(filled[:, None], tokens[source_row], zero_value).reshape(
        experts_all, capacity, model_width
    )
    cot_buf = jnp.where(filled[:, None], cotangent[source_row], zero_value).reshape(
        experts_all, capacity, model_width
    )
    weight_buf = (
        jnp.where(filled, route_weight.reshape(-1)[entry], 0.0)
        .astype(jnp.bfloat16)
        .reshape(experts_all, capacity)
    )
    start = lax.axis_index("tp") * shard_width
    token_part = lax.dynamic_slice_in_dim(token_buf, start, shard_width, 2)
    cot_part = lax.dynamic_slice_in_dim(cot_buf, start, shard_width, 2)
    token_part, cot_part, arrived_weight = (
        lax.all_to_all(token_part, "ep", split_axis=0, concat_axis=1, tiled=True),
        lax.all_to_all(cot_part, "ep", split_axis=0, concat_axis=1, tiled=True),
        lax.all_to_all(weight_buf, "ep", split_axis=0, concat_axis=1, tiled=True),
    )
    arrived_tokens, arrived_cot = (
        lax.all_gather(token_part, "tp", axis=2, tiled=True),
        lax.all_gather(cot_part, "tp", axis=2, tiled=True),
    )
    gate_pre = jnp.einsum(
        "erd,edf->erf", arrived_tokens, gate_weight, preferred_element_type=jnp.float32
    )
    up_pre = jnp.einsum(
        "erd,edf->erf", arrived_tokens, up_weight, preferred_element_type=jnp.float32
    )
    sig = jax.nn.sigmoid(gate_pre)
    active = gate_pre * sig
    hidden = (active * up_pre).astype(jnp.bfloat16)
    back_raw = jnp.einsum(
        "erd,efd->erf", arrived_cot, down_weight, preferred_element_type=jnp.float32
    )
    route_part = jnp.sum(hidden.astype(jnp.float32) * back_raw, axis=2)
    slot_weight = arrived_weight.astype(jnp.float32)
    scaled_back = slot_weight[:, :, None] * back_raw
    grad_gate_pre = (scaled_back * up_pre * sig * (1.0 + gate_pre * (1.0 - sig))).astype(
        jnp.bfloat16
    )
    grad_up_pre = (scaled_back * active).astype(jnp.bfloat16)
    scaled_cot = (slot_weight[:, :, None] * arrived_cot).astype(jnp.bfloat16)
    grad_gate = jnp.einsum(
        "erd,erf->edf", arrived_tokens, grad_gate_pre, preferred_element_type=jnp.float32
    ).astype(jnp.bfloat16)
    grad_up = jnp.einsum(
        "erd,erf->edf", arrived_tokens, grad_up_pre, preferred_element_type=jnp.float32
    ).astype(jnp.bfloat16)
    grad_down = jnp.einsum(
        "erf,erd->efd", hidden, scaled_cot, preferred_element_type=jnp.float32
    ).astype(jnp.bfloat16)
    row_part = jnp.einsum(
        "erf,edf->erd", grad_gate_pre, gate_weight, preferred_element_type=jnp.float32
    )
    row_part = row_part + jnp.einsum(
        "erf,edf->erd", grad_up_pre, up_weight, preferred_element_type=jnp.float32
    )
    row_summed = lax.psum_scatter(
        row_part.astype(jnp.bfloat16), "tp", scatter_dimension=2, tiled=True
    )
    returned = lax.all_to_all(row_summed, "ep", split_axis=1, concat_axis=0, tiled=True)
    route_total = lax.psum(route_part, "tp")
    route_back = lax.all_to_all(route_total, "ep", split_axis=1, concat_axis=0, tiled=True)
    per_entry = returned.reshape(experts_all * capacity, shard_width)[slot_index]
    grad_tokens = jnp.sum(
        per_entry.astype(jnp.float32).reshape(rows, top, shard_width), axis=1
    ).astype(jnp.bfloat16)
    grad_route = route_back.reshape(-1)[slot_index].reshape(rows, top)
    return (grad_tokens, grad_route, grad_gate, grad_up, grad_down)


def step_kernel(
    n_ep, n_tp,
    x_hbm, c_hbm, routes_hbm, weight_hbm, wg_hbm, wu_hbm, wd_hbm,
    gt_ref, rt_ref, gg, gu, hid, sc,
    routes_ref, weight_ref, wgt, wut, wdt, xc, wt, wg, wu, wd, da, db, rp, pr, r1, r2, zr, rcol, rm, rr, ra, rb,
    zq, rq, s_zf, r_zf, s_rq, r_rq, lsem, s_fwd, r_fwd, s_pair, r_pair, s_rp, r_rp, s_xy, r_xy, s_z, r_z, s_rt, r_rt,
):
    nz = n_tp // 2
    hz = nz // 2
    rows, width = x_hbm.shape
    hidden_units = wg.shape[1]
    shard = width // n_tp
    piece = rows // (nz + 2)
    ends = (0, 2 * piece, 3 * piece, 4 * piece, rows)
    groups = ((0, 2 * piece), (2 * piece, 2 * piece), (4 * piece, rows - 4 * piece))
    cuts = (0, 2 * piece, 4 * piece, rows - piece, rows)
    p, t = lax.axis_index("ep"), lax.axis_index("tp")
    k, z = t % 2, t // 2
    px, py, pd = p + 1 - 2 * (p % 2), p + 2 - 4 * (p // 2), 3 - p
    mate = t + 1 - 2 * k

    def remote(src, dst, send, recv, ep, tp):
        return pltpu.make_async_remote_copy(
            src_ref=src, dst_ref=dst, send_sem=send, recv_sem=recv,
            device_id={"ep": ep, "tp": tp}, device_id_type=pl.DeviceIdType.MESH,
        )

    local = [
        pltpu.make_async_copy(x_hbm, xc.at[p, pl.ds(0, rows)], lsem.at[0]),
        pltpu.make_async_copy(c_hbm, xc.at[p, pl.ds(rows, rows)], lsem.at[1]),
        pltpu.make_async_copy(routes_hbm, routes_ref, lsem.at[5]),
        pltpu.make_async_copy(weight_hbm, weight_ref, lsem.at[6]),
        pltpu.make_async_copy(wg_hbm, wg, lsem.at[2]),
        pltpu.make_async_copy(wu_hbm, wu, lsem.at[3]),
        pltpu.make_async_copy(wd_hbm, wd, lsem.at[4]),
    ]
    for copy in local:
        copy.start()
    barrier = pltpu.get_barrier_semaphore()
    for other in (px, py, pd):
        pl.semaphore_signal(barrier, inc=1, device_id={"ep": other, "tp": t}, device_id_type=pl.DeviceIdType.MESH)
    for step in range(1, n_tp):
        pl.semaphore_signal(barrier, inc=1, device_id={"ep": p, "tp": (t + step) % n_tp}, device_id_type=pl.DeviceIdType.MESH)
    for copy in local[2:4]:
        copy.wait()
    experts = lax.broadcasted_iota(jnp.int32, (8, rows), 0)
    mixed = jnp.zeros((8, rows), F32)
    for choice in range(routes_ref.shape[0]):
        hit = routes_ref[choice:choice + 1, :] == experts
        mixed = mixed + jnp.where(hit, weight_ref[choice:choice + 1, :], 0.0)
    wt[p] = jnp.zeros(wt.shape[1:], F32)
    wt[p, :, 0:rows] = mixed.astype(BF16).astype(F32)
    pl.semaphore_wait(barrier, n_ep - 1 + n_tp - 1)
    for copy in local[:2]:
        copy.wait()

    sends = []

    def go(copy):
        copy.start()
        sends.append(copy)

    def sub_rows(half, lower, count):
        return pl.ds(pl.multiple_of(half * rows + lower, 16), count)

    def piece_rows(half, owner):
        return sub_rows(half, (2 + owner) * piece, piece)

    def half_rows(half, part):
        return sub_rows(half, ends[part], ends[part + 1] - ends[part])

    def span_of(chunk):
        return pl.ds(cuts[chunk], cuts[chunk + 1] - cuts[chunk])

    for at, other in enumerate((pd, px, py)):
        go(remote(wt.at[p], wt.at[p], s_fwd.at[at], r_fwd.at[at], other, t))
    mine = xc.at[p, piece_rows(k, z)]
    go(remote(mine, mine, s_fwd.at[3], r_fwd.at[3], pd, t))

    def send_near(part):
        for at, other in enumerate((px, py)):
            sem = 4 + 2 * part + at
            mine = xc.at[p, half_rows(k, part)]
            go(remote(mine, mine, s_fwd.at[sem], r_fwd.at[sem], other, t))

    send_near(0)
    send_near(1)

    def arrived(ref, send, recv):
        remote(ref, ref, send, recv, p, mate).wait_recv()

    for copy in local[4:]:
        copy.wait()
    tn = (((0,), (0,)), ((), ()))

    def weights_of(b):
        at_expert = lax.broadcasted_iota(jnp.int32, wt.shape[1:], 0) == p
        row = jnp.sum(jnp.where(at_expert, wt[b], 0.0), axis=0, keepdims=True)
        return jnp.broadcast_to(row, (128, LANES)).T[:, 0:1]

    def compute(parts, between=None):
        count = sum(size for _, _, size in parts)

        def load(ref, shift, cols):
            got = [ref[b, pl.ds(shift + lower, size), cols] for b, lower, size in parts]
            return got[0] if len(got) == 1 else jnp.concatenate(got, axis=0)

        def store(ref, cols, value):
            done = 0
            for b, lower, size in parts:
                ref[b, pl.ds(lower, size), cols] = value[done:done + size]
                done += size

        every = slice(None)
        weight = [weights_of(b)[lower:lower + size] for b, lower, size in parts]
        weight = weight[0] if len(weight) == 1 else jnp.concatenate(weight, axis=0)
        tile = min(hidden_units, 256)
        route, das, dbs = jnp.zeros((count, 1), F32), [], []
        for at in range(hidden_units // tile):
            cols = pl.ds(at * tile, tile)
            x = load(xc, 0, every)
            gate = jnp.dot(x, wg[:, cols], preferred_element_type=F32)
            up = jnp.dot(x, wu[:, cols], preferred_element_type=F32)
            back = jnp.dot(load(xc, rows, every), wdt[:, cols], preferred_element_type=F32)
            sig = jax.nn.sigmoid(gate)
            active = gate * sig
            hidden = (active * up).astype(BF16)
            store(hid, cols, hidden)
            route = route + jnp.sum(hidden.astype(F32) * back, axis=1, keepdims=True)
            scaled = weight * back
            das.append((scaled * up * sig * (1.0 + gate * (1.0 - sig))).astype(BF16))
            dbs.append((scaled * active).astype(BF16))
            store(da, cols, das[-1])
            store(db, cols, dbs[-1])
        store(rcol, every, jnp.broadcast_to(route, (count, 128)))
        if between is not None:
            between()
        for at in range(nz):
            cols = pl.ds(2 * at * shard, 2 * shard)
            part = None
            for up_to, (left, right) in enumerate(zip(das, dbs)):
                units = pl.ds(up_to * tile, tile)
                term = jnp.dot(left, wgt[units, cols], preferred_element_type=F32)
                part = term if part is None else part + term
                part = part + jnp.dot(right, wut[units, cols], preferred_element_type=F32)
            part, done = part.astype(BF16), 0
            for b, lower, size in parts:
                for core in range(2):
                    rp[core, at, b, pl.ds(lower, size), :] = part[done:done + size, core * shard:(core + 1) * shard]
                done += size
        for b, lower, size in parts:
            for chunk in range(CHUNKS):
                if not lower <= cuts[chunk] < lower + size:
                    continue
                span = span_of(chunk)
                sem = CHUNKS * orders[id(b)] + chunk
                go(remote(rp.at[1 - k, :, b, span], pr.at[:, b, span], s_rp.at[sem], r_rp.at[sem], p, mate))
        store(sc, every, (weight * load(xc, rows, every).astype(F32)).astype(BF16))

    orders = {id(p): 0, id(px): 1, id(py): 2, id(pd): 3}
    def add_pair(b, chunk):
        span = span_of(chunk)
        sem = CHUNKS * orders[id(b)] + chunk
        arrived(pr.at[:, b, span], s_rp.at[sem], r_rp.at[sem])
        for at in range(nz):
            rp[k, at, b, span, :] = (rp[k, at, b, span, :].astype(F32) + pr[at, b, span, :].astype(F32)).astype(BF16)

    def z_first(b):
        add_pair(b, 0)
        for step in range(1, nz):
            sem = orders[id(b)] * nz + step
            go(remote(
                rp.at[k, (z + step) % nz, b, span_of(0)], zq.at[step, orders[id(b)]],
                s_zf.at[sem], r_zf.at[sem], p, (t + 2 * step) % n_tp,
            ))

    def z_sum(b):
        at, span = orders[id(b)], span_of(0)
        total = rp[k, z, b, span, :].astype(F32)
        for step in range(1, nz):
            sem = at * nz + step
            arrived(zq.at[step, at], s_zf.at[sem], r_zf.at[sem])
            total = total + zq[step, at].astype(F32)
        rp[k, z, b, span, :] = total.astype(BF16)
        if at:
            go(remote(rp.at[k, z, b, span], rq.at[at - 1], s_rq.at[at - 1], r_rq.at[at - 1], b, t))

    def xy_sem(at, kind, chunk):
        return (kind * nz + at) * CHUNKS + chunk

    def first(at, b, kind, other, chunk):
        span = span_of(chunk)
        sem = xy_sem(at, kind, chunk)
        go(remote(rp.at[k, at, b, span], r1.at[at, kind, span], s_xy.at[sem], r_xy.at[sem], other, t))

    def first_near(chunk):
        add_pair(px, chunk)
        add_pair(py, chunk)
        for at in range(hz):
            first(at, px, 0, px, chunk)
            first(hz + at, py, 0, py, chunk)

    def first_pd(chunks):
        for chunk in chunks:
            add_pair(pd, chunk)
            for at in range(hz):
                first(at, pd, 1, px, chunk)
                first(hz + at, pd, 1, py, chunk)

    def second(at, b, other, chunk):
        span = span_of(chunk)
        sem = xy_sem(at, 1, chunk)
        arrived(r1.at[at, 1, span], s_xy.at[sem], r_xy.at[sem])
        rp[k, at, b, span, :] = (rp[k, at, b, span, :].astype(F32) + r1[at, 1, span, :].astype(F32)).astype(BF16)
        sem = xy_sem(at, 2, chunk)
        go(remote(rp.at[k, at, b, span], r2.at[at, span], s_xy.at[sem], r_xy.at[sem], other, t))

    def take_near(part):
        for at, other in enumerate((px, py)):
            mine = xc.at[other, half_rows(k, part)]
            sem = 4 + 2 * part + at
            arrived(mine, s_fwd.at[sem], r_fwd.at[sem])
            go(remote(mine, mine, s_pair.at[sem], r_pair.at[sem], p, mate))

    def wait_near(part):
        for at, other in enumerate((px, py)):
            sem = 4 + 2 * part + at
            arrived(xc.at[other, half_rows(1 - k, part)], s_pair.at[sem], r_pair.at[sem])

    def compute_near(group, between=None):
        lower, size = groups[group]
        compute([(px, lower, size), (py, lower, size)], between)

    for at in range(width // 512):
        for to in range(hidden_units // 256):
            a, b = pl.ds(at * 512, 512), pl.ds(to * 256, 256)
            wgt[b, a] = wg[a, b].T
            wut[b, a] = wu[a, b].T
            wdt[a, b] = wd[b, a].T
    compute([(p, 0, rows)])
    mine = xc.at[pd, piece_rows(k, z)]
    arrived(mine, s_fwd.at[3], r_fwd.at[3])
    for step in range(1, nz):
        go(remote(mine, mine, s_z.at[step], r_z.at[step], p, (t + 2 * step) % n_tp))
    go(remote(mine, mine, s_pair.at[0], r_pair.at[0], p, mate))
    take_near(0)
    for at, other in enumerate((px, py)):
        passed = xc.at[other, sub_rows(k, at * piece, piece)]
        sem = 4 + 2 * PARTS + at
        go(remote(passed, passed, s_fwd.at[sem], r_fwd.at[sem], py if at == 0 else px, t))
    send_near(2)
    send_near(3)
    for chunk in range(1, CHUNKS):
        add_pair(p, chunk)
    arrived(wt.at[pd], s_fwd.at[0], r_fwd.at[0])
    arrived(wt.at[px], s_fwd.at[1], r_fwd.at[1])
    arrived(wt.at[py], s_fwd.at[2], r_fwd.at[2])
    wait_near(0)
    compute_near(0)
    take_near(1)
    for step in range(1, nz):
        mine = xc.at[pd, piece_rows(k, (z - step + nz) % nz)]
        arrived(mine, s_z.at[step], r_z.at[step])
        go(remote(mine, mine, s_pair.at[step], r_pair.at[step], p, mate))
    for at in range(2):
        sem = 4 + 2 * PARTS + at
        passed = xc.at[pd, sub_rows(k, at * piece, piece)]
        arrived(passed, s_fwd.at[sem], r_fwd.at[sem])
        go(remote(passed, passed, s_pair.at[sem], r_pair.at[sem], p, mate))
    z_first(p)
    z_first(px)
    z_first(py)
    for at in range(2):
        sem = 4 + 2 * PARTS + at
        arrived(xc.at[pd, sub_rows(1 - k, at * piece, piece)], s_pair.at[sem], r_pair.at[sem])
    for step in range(nz):
        arrived(xc.at[pd, piece_rows(1 - k, (z - step + nz) % nz)], s_pair.at[step], r_pair.at[step])
    compute([(pd, 0, rows)], lambda: take_near(2))
    wait_near(1)
    wait_near(2)

    def send_far():
        first_pd(range(1, CHUNKS))
        z_first(pd)

    compute_near(1, send_far)
    z_sum(p)
    take_near(3)
    first_near(1)

    def second_both(chunk):
        for at in range(hz):
            second(at, py, py, chunk)
            second(hz + at, px, px, chunk)

    wait_near(3)
    compute_near(2, lambda: second_both(1))

    def wide(ref, lower, count, cols):
        got = ref[:, pl.ds(lower, count), cols]
        return got.reshape(n_ep * count, got.shape[2])

    def up_grads(*slices):
        for at in slices:
            cols = pl.ds(at * (width // 8), width // 8)
            left = wide(xc, 0, rows, cols)
            for grads, out in ((da, gg), (db, gu)):
                out[cols, :] = lax.dot_general(
                    left, wide(grads, 0, rows, slice(None)), tn, preferred_element_type=F32
                ).astype(BF16)

    def third(chunk):
        span = span_of(chunk)
        for at in range(nz):
            for kind, ref in ((0, r1.at[at, 0, span]), (2, r2.at[at, span])):
                sem = xy_sem(at, kind, chunk)
                arrived(ref, s_xy.at[sem], r_xy.at[sem])
            mine = rp[k, at, p, span, :].astype(F32) + r1[at, 0, span, :].astype(F32) + r2[at, span, :].astype(F32)
            rp[k, at, p, span, :] = mine.astype(BF16)
        for step in range(1, nz):
            sem = (1 + chunk) * nz + step
            go(remote(rp.at[k, (z + step) % nz, p, span], zr.at[step, span], s_z.at[sem], r_z.at[sem], p, (t + 2 * step) % n_tp))

    def send_route():
        for b in range(n_ep):
            rm[b:b + 1, :] = rcol[b].T[0:1, :]
        for step in range(1, n_tp):
            go(remote(rm, rr.at[step], s_rt.at[step], r_rt.at[step], p, (t + step) % n_tp))

    def return_route():
        total = rm[...]
        for step in range(1, n_tp):
            arrived(rr.at[step], s_rt.at[step], r_rt.at[step])
            total = total + rr[step]
        ra[...] = total
        for at, other in enumerate((px, py, pd)):
            go(remote(ra, rb.at[at], s_rt.at[n_tp + at], r_rt.at[n_tp + at], other, t))

    send_route()
    up_grads(0, 1)
    for chunk in range(2, CHUNKS):
        first_near(chunk)
        second_both(chunk)
    third(1)
    up_grads(2, 3)
    z_sum(px)
    z_sum(py)
    z_sum(pd)
    up_grads(4)
    return_route()
    up_grads(5)
    third(2)
    up_grads(6)
    third(3)
    up_grads(7)

    index = lax.broadcasted_iota(jnp.int32, rm.shape, 0)
    result = jnp.zeros(rm.shape, F32)
    for at, other in enumerate((px, py, pd, p)):
        if at < 3:
            arrived(rb.at[at], s_rt.at[n_tp + at], r_rt.at[n_tp + at])
        got = rb[at] if at < 3 else ra[...]
        row = jnp.sum(jnp.where(index == p, got, 0.0), axis=0, keepdims=True)
        result = result + jnp.where(index == other, row, 0.0)
    for choice in range(routes_ref.shape[0]):
        hit = routes_ref[choice:choice + 1, :] == experts
        rt_ref[choice:choice + 1, :] = jnp.sum(jnp.where(hit, result[:, 0:rows], 0.0), axis=0, keepdims=True)

    total = rp[k, z, p, span_of(0), :].astype(F32)
    for at in range(3):
        arrived(rq.at[at], s_rq.at[at], r_rq.at[at])
        total = total + rq[at].astype(F32)
    gt_ref[span_of(0), :] = total.astype(BF16)
    for chunk in range(1, CHUNKS):
        span = span_of(chunk)
        total = rp[k, z, p, span, :].astype(F32)
        for step in range(1, nz):
            sem = (1 + chunk) * nz + step
            arrived(zr.at[step, span], s_z.at[sem], r_z.at[sem])
            total = total + zr[step, span, :].astype(F32)
        gt_ref[span, :] = total.astype(BF16)
    for copy in sends:
        copy.wait_send()


def write_kernel(gt, rt, gg, gu, hid, sc, gt_hbm, rt_hbm, gg_hbm, gu_hbm, gd_hbm, gd, sem):
    pairs = ((gt, gt_hbm), (rt, rt_hbm), (gg, gg_hbm), (gu, gu_hbm))
    copies = [pltpu.make_async_copy(left, right, sem.at[at]) for at, (left, right) in enumerate(pairs)]
    units, width = gd.shape
    merged = hid.shape[0] * hid.shape[1]
    for copy in copies:
        copy.start()
    for at in range(4):
        cols = pl.ds(at * (width // 4), width // 4)
        gd[:, cols] = lax.dot_general(
            hid[...].reshape(merged, units), sc[:, :, cols].reshape(merged, width // 4),
            (((0,), (0,)), ((), ())), preferred_element_type=F32,
        ).astype(BF16)
        copies.append(pltpu.make_async_copy(gd.at[:, cols], gd_hbm.at[:, cols], sem.at[4 + at]))
        copies[-1].start()
    for copy in copies:
        copy.wait()


def fused(n_ep, n_tp, tokens, cotangent, routes, route_weight, gate_weight, up_weight, down_weight):
    rows, width = tokens.shape
    units = gate_weight.shape[2]
    nz = n_tp // 2
    shard = width // n_tp
    hbm, vmem = pl.BlockSpec(memory_space=pltpu.HBM), pl.BlockSpec(memory_space=pltpu.VMEM)
    dma = pltpu.SemaphoreType.DMA
    results = pl.pallas_call(
        functools.partial(step_kernel, n_ep, n_tp),
        out_shape=(
            jax.ShapeDtypeStruct((rows, shard), BF16),
            jax.ShapeDtypeStruct((routes.shape[1], rows), F32),
            jax.ShapeDtypeStruct((width, units), BF16),
            jax.ShapeDtypeStruct((width, units), BF16),
            jax.ShapeDtypeStruct((n_ep, rows, units), BF16),
            jax.ShapeDtypeStruct((n_ep, rows, width), BF16),
        ),
        in_specs=[hbm] * 7,
        out_specs=(vmem,) * 6,
        scratch_shapes=[
            pltpu.VMEM((routes.shape[1], rows), jnp.int32),
            pltpu.VMEM((routes.shape[1], rows), F32),
            pltpu.VMEM((units, width), BF16),
            pltpu.VMEM((units, width), BF16),
            pltpu.VMEM((width, units), BF16),
            pltpu.VMEM((n_ep, 2 * rows, width), BF16),
            pltpu.VMEM((n_ep, 8, LANES), F32),
            pltpu.VMEM((width, units), BF16),
            pltpu.VMEM((width, units), BF16),
            pltpu.VMEM((units, width), BF16),
            pltpu.VMEM((n_ep, rows, units), BF16),
            pltpu.VMEM((n_ep, rows, units), BF16),
            pltpu.VMEM((2, nz, n_ep, rows, shard), BF16),
            pltpu.VMEM((nz, n_ep, rows, shard), BF16),
            pltpu.VMEM((nz, 2, rows, shard), BF16),
            pltpu.VMEM((nz, rows, shard), BF16),
            pltpu.VMEM((nz, rows, shard), BF16),
            pltpu.VMEM((n_ep, LANES, 128), F32),
            pltpu.VMEM((8, LANES), F32),
            pltpu.VMEM((n_tp, 8, LANES), F32),
            pltpu.VMEM((8, LANES), F32),
            pltpu.VMEM((3, 8, LANES), F32),
            pltpu.VMEM((nz, n_ep, 2 * (rows // (nz + 2)), shard), BF16),
            pltpu.VMEM((3, 2 * (rows // (nz + 2)), shard), BF16),
            dma((n_ep * nz,)),
            dma((n_ep * nz,)),
            dma((3,)),
            dma((3,)),
            dma((7,)),
            dma((6 + 2 * PARTS,)),
            dma((6 + 2 * PARTS,)),
            dma((6 + 2 * PARTS,)),
            dma((6 + 2 * PARTS,)),
            dma((n_ep * CHUNKS,)),
            dma((n_ep * CHUNKS,)),
            dma((3 * nz * CHUNKS,)),
            dma((3 * nz * CHUNKS,)),
            dma(((1 + CHUNKS) * nz,)),
            dma(((1 + CHUNKS) * nz,)),
            dma((n_tp + 3,)),
            dma((n_tp + 3,)),
        ],
        compiler_params=pltpu.CompilerParams(
            collective_id=0, has_side_effects=True, vmem_limit_bytes=VLIM * 1024 * 1024
        ),
    )(*(pltpu.with_memory_space_constraint(array, pltpu.HBM) for array in (
        tokens, cotangent, routes.T, route_weight.T, gate_weight[0], up_weight[0], down_weight[0]
    )))
    grad_tokens, by_choice, grad_gate, grad_up, grad_down = pl.pallas_call(
        write_kernel,
        out_shape=tuple(jax.ShapeDtypeStruct(array.shape, array.dtype) for array in results[:4])
        + (jax.ShapeDtypeStruct((units, width), BF16),),
        in_specs=[vmem] * 6,
        out_specs=(hbm,) * 5,
        scratch_shapes=[pltpu.VMEM((units, width), BF16), dma((8,))],
        compiler_params=pltpu.CompilerParams(vmem_limit_bytes=8 * 1024 * 1024),
    )(*results)
    grad_route = by_choice.T
    return grad_tokens, grad_route, grad_gate[None], grad_up[None], grad_down[None]


def body(mesh, *arrays):
    n_ep, n_tp = mesh.shape["ep"], mesh.shape["tp"]
    rows, width = arrays[0].shape
    experts, _, units = arrays[4].shape
    capacity = 2 * rows * arrays[2].shape[1] // (experts * n_ep)
    fits = (
        n_ep == 4 and experts == 1 and n_tp == 8 and capacity >= rows and rows <= LANES
        and width % (n_tp * 128) == 0 and width % 512 == 0 and units % 256 == 0
        and units >= 512 and width % 1024 == 0 and rows % (16 * (n_tp // 2 + 2)) == 0
    )
    return fused(n_ep, n_tp, *arrays) if fits else shards(*arrays)


def solution(mesh):
    return jax.shard_map(
        functools.partial(body, mesh),
        mesh=mesh,
        in_specs=(
            P("ep", None),
            P("ep", None),
            P("ep", None),
            P("ep", None),
            P("ep", None, "tp"),
            P("ep", None, "tp"),
            P("ep", "tp", None),
        ),
        out_specs=(
            P("ep", "tp"),
            P("ep", None),
            P("ep", None, "tp"),
            P("ep", None, "tp"),
            P("ep", "tp", None),
        ),
        check_vma=False,
    )
```

```python
import functools

import jax
import jax.numpy as jnp
from jax import lax
from jax.experimental import pallas as pl
from jax.experimental.pallas import tpu as pltpu
from jax.sharding import PartitionSpec as P

F32, BF16 = jnp.float32, jnp.bfloat16
LANES = 256
CHUNKS = 4
PARTS = 4
VLIM = 40


def shards(tokens, cotangent, routes, route_weight, gate_weight, up_weight, down_weight):
    rows, model_width = tokens.shape
    top = routes.shape[1]
    local_experts = gate_weight.shape[0]
    experts_all = local_experts * lax.axis_size("ep")
    capacity = 2 * rows * top // experts_all
    shard_width = model_width // lax.axis_size("tp")
    flat_routes = routes.reshape(-1)
    expert_ids = jnp.arange(experts_all, dtype=jnp.int32)
    onehot_table = (flat_routes[:, None] == expert_ids[None, :]).astype(jnp.int32)
    earlier = jnp.cumsum(onehot_table, axis=0) - onehot_table
    order_in = jnp.sum(earlier * onehot_table, axis=1)
    slot_index = flat_routes * capacity + order_in
    entries = jnp.arange(rows * top, dtype=jnp.int32) + 1
    slot_table = jnp.zeros((experts_all * capacity,), jnp.int32).at[slot_index].set(entries)
    filled = slot_table > 0
    entry = jnp.maximum(slot_table - 1, 0)
    source_row = entry // top
    zero_value = jnp.zeros((), jnp.bfloat16)
    token_buf = jnp.where(filled[:, None], tokens[source_row], zero_value).reshape(
        experts_all, capacity, model_width
    )
    cot_buf = jnp.where(filled[:, None], cotangent[source_row], zero_value).reshape(
        experts_all, capacity, model_width
    )
    weight_buf = (
        jnp.where(filled, route_weight.reshape(-1)[entry], 0.0)
        .astype(jnp.bfloat16)
        .reshape(experts_all, capacity)
    )
    start = lax.axis_index("tp") * shard_width
    token_part = lax.dynamic_slice_in_dim(token_buf, start, shard_width, 2)
    cot_part = lax.dynamic_slice_in_dim(cot_buf, start, shard_width, 2)
    token_part, cot_part, arrived_weight = (
        lax.all_to_all(token_part, "ep", split_axis=0, concat_axis=1, tiled=True),
        lax.all_to_all(cot_part, "ep", split_axis=0, concat_axis=1, tiled=True),
        lax.all_to_all(weight_buf, "ep", split_axis=0, concat_axis=1, tiled=True),
    )
    arrived_tokens, arrived_cot = (
        lax.all_gather(token_part, "tp", axis=2, tiled=True),
        lax.all_gather(cot_part, "tp", axis=2, tiled=True),
    )
    gate_pre = jnp.einsum(
        "erd,edf->erf", arrived_tokens, gate_weight, preferred_element_type=jnp.float32
    )
    up_pre = jnp.einsum(
        "erd,edf->erf", arrived_tokens, up_weight, preferred_element_type=jnp.float32
    )
    sig = jax.nn.sigmoid(gate_pre)
    active = gate_pre * sig
    hidden = (active * up_pre).astype(jnp.bfloat16)
    back_raw = jnp.einsum(
        "erd,efd->erf", arrived_cot, down_weight, preferred_element_type=jnp.float32
    )
    route_part = jnp.sum(hidden.astype(jnp.float32) * back_raw, axis=2)
    slot_weight = arrived_weight.astype(jnp.float32)
    scaled_back = slot_weight[:, :, None] * back_raw
    grad_gate_pre = (scaled_back * up_pre * sig * (1.0 + gate_pre * (1.0 - sig))).astype(
        jnp.bfloat16
    )
    grad_up_pre = (scaled_back * active).astype(jnp.bfloat16)
    scaled_cot = (slot_weight[:, :, None] * arrived_cot).astype(jnp.bfloat16)
    grad_gate = jnp.einsum(
        "erd,erf->edf", arrived_tokens, grad_gate_pre, preferred_element_type=jnp.float32
    ).astype(jnp.bfloat16)
    grad_up = jnp.einsum(
        "erd,erf->edf", arrived_tokens, grad_up_pre, preferred_element_type=jnp.float32
    ).astype(jnp.bfloat16)
    grad_down = jnp.einsum(
        "erf,erd->efd", hidden, scaled_cot, preferred_element_type=jnp.float32
    ).astype(jnp.bfloat16)
    row_part = jnp.einsum(
        "erf,edf->erd", grad_gate_pre, gate_weight, preferred_element_type=jnp.float32
    )
    row_part = row_part + jnp.einsum(
        "erf,edf->erd", grad_up_pre, up_weight, preferred_element_type=jnp.float32
    )
    row_summed = lax.psum_scatter(
        row_part.astype(jnp.bfloat16), "tp", scatter_dimension=2, tiled=True
    )
    returned = lax.all_to_all(row_summed, "ep", split_axis=1, concat_axis=0, tiled=True)
    route_total = lax.psum(route_part, "tp")
    route_back = lax.all_to_all(route_total, "ep", split_axis=1, concat_axis=0, tiled=True)
    per_entry = returned.reshape(experts_all * capacity, shard_width)[slot_index]
    grad_tokens = jnp.sum(
        per_entry.astype(jnp.float32).reshape(rows, top, shard_width), axis=1
    ).astype(jnp.bfloat16)
    grad_route = route_back.reshape(-1)[slot_index].reshape(rows, top)
    return (grad_tokens, grad_route, grad_gate, grad_up, grad_down)


def step_kernel(
    n_ep, n_tp,
    x_hbm, c_hbm, routes_hbm, weight_hbm, wg_hbm, wu_hbm, wd_hbm,
    gt_ref, rt_ref, gg, gu, hid, sc,
    routes_ref, weight_ref, wgt, wut, wdt, xc, wt, wg, wu, wd, da, db, rp, pr, r1, r2, zr, rcol, rm, rr, ra, rb,
    zq, rq, s_zf, r_zf, s_rq, r_rq, lsem, s_fwd, r_fwd, s_pair, r_pair, s_rp, r_rp, s_xy, r_xy, s_z, r_z, s_rt, r_rt,
):
    nz = n_tp // 2
    hz = nz // 2
    rows, width = x_hbm.shape
    hidden_units = wg.shape[1]
    shard = width // n_tp
    piece = rows // (nz + 2)
    ends = (0, 2 * piece, 3 * piece, 4 * piece, rows)
    groups = ((0, 2 * piece), (2 * piece, 2 * piece), (4 * piece, rows - 4 * piece))
    cuts = (0, 2 * piece, 4 * piece, rows - piece, rows)
    p, t = lax.axis_index("ep"), lax.axis_index("tp")
    k, z = t % 2, t // 2
    px, py, pd = p + 1 - 2 * (p % 2), p + 2 - 4 * (p // 2), 3 - p
    mate = t + 1 - 2 * k

    def remote(src, dst, send, recv, ep, tp):
        return pltpu.make_async_remote_copy(
            src_ref=src, dst_ref=dst, send_sem=send, recv_sem=recv,
            device_id={"ep": ep, "tp": tp}, device_id_type=pl.DeviceIdType.MESH,
        )

    local = [
        pltpu.make_async_copy(x_hbm, xc.at[p, pl.ds(0, rows)], lsem.at[0]),
        pltpu.make_async_copy(c_hbm, xc.at[p, pl.ds(rows, rows)], lsem.at[1]),
        pltpu.make_async_copy(routes_hbm, routes_ref, lsem.at[5]),
        pltpu.make_async_copy(weight_hbm, weight_ref, lsem.at[6]),
        pltpu.make_async_copy(wg_hbm, wg, lsem.at[2]),
        pltpu.make_async_copy(wu_hbm, wu, lsem.at[3]),
        pltpu.make_async_copy(wd_hbm, wd, lsem.at[4]),
    ]
    for copy in local:
        copy.start()
    barrier = pltpu.get_barrier_semaphore()
    for other in (px, py, pd):
        pl.semaphore_signal(barrier, inc=1, device_id={"ep": other, "tp": t}, device_id_type=pl.DeviceIdType.MESH)
    for step in range(1, n_tp):
        pl.semaphore_signal(barrier, inc=1, device_id={"ep": p, "tp": (t + step) % n_tp}, device_id_type=pl.DeviceIdType.MESH)
    for copy in local[2:4]:
        copy.wait()
    experts = lax.broadcasted_iota(jnp.int32, (8, rows), 0)
    mixed = jnp.zeros((8, rows), F32)
    for choice in range(routes_ref.shape[0]):
        hit = routes_ref[choice:choice + 1, :] == experts
        mixed = mixed + jnp.where(hit, weight_ref[choice:choice + 1, :], 0.0)
    wt[p] = jnp.zeros(wt.shape[1:], F32)
    wt[p, :, 0:rows] = mixed.astype(BF16).astype(F32)
    pl.semaphore_wait(barrier, n_ep - 1 + n_tp - 1)
    for copy in local[:2]:
        copy.wait()

    sends = []

    def go(copy):
        copy.start()
        sends.append(copy)

    def sub_rows(half, lower, count):
        return pl.ds(pl.multiple_of(half * rows + lower, 16), count)

    def piece_rows(half, owner):
        return sub_rows(half, (2 + owner) * piece, piece)

    def half_rows(half, part):
        return sub_rows(half, ends[part], ends[part + 1] - ends[part])

    def span_of(chunk):
        return pl.ds(cuts[chunk], cuts[chunk + 1] - cuts[chunk])

    for at, other in enumerate((pd, px, py)):
        go(remote(wt.at[p], wt.at[p], s_fwd.at[at], r_fwd.at[at], other, t))
    mine = xc.at[p, piece_rows(1 - k, z)]
    go(remote(mine, mine, s_fwd.at[3], r_fwd.at[3], pd, t))

    def send_near(part):
        for at, other in enumerate((px, py)):
            sem = 4 + 2 * part + at
            mine = xc.at[p, half_rows(1 - k, part)]
            go(remote(mine, mine, s_fwd.at[sem], r_fwd.at[sem], other, t))

    send_near(0)
    send_near(1)

    def arrived(ref, send, recv):
        remote(ref, ref, send, recv, p, mate).wait_recv()

    for copy in local[4:]:
        copy.wait()
    tn = (((0,), (0,)), ((), ()))

    def weights_of(b):
        at_expert = lax.broadcasted_iota(jnp.int32, wt.shape[1:], 0) == p
        row = jnp.sum(jnp.where(at_expert, wt[b], 0.0), axis=0, keepdims=True)
        return jnp.broadcast_to(row, (128, LANES)).T[:, 0:1]

    def compute(parts, between=None):
        count = sum(size for _, _, size in parts)

        def load(ref, shift, cols):
            got = [ref[b, pl.ds(shift + lower, size), cols] for b, lower, size in parts]
            return got[0] if len(got) == 1 else jnp.concatenate(got, axis=0)

        def store(ref, cols, value):
            done = 0
            for b, lower, size in parts:
                ref[b, pl.ds(lower, size), cols] = value[done:done + size]
                done += size

        every = slice(None)
        weight = [weights_of(b)[lower:lower + size] for b, lower, size in parts]
        weight = weight[0] if len(weight) == 1 else jnp.concatenate(weight, axis=0)
        tile = min(hidden_units, 256)
        route, das, dbs = jnp.zeros((count, 1), F32), [], []
        for at in range(hidden_units // tile):
            cols = pl.ds(at * tile, tile)
            x = load(xc, 0, every)
            gate = jnp.dot(x, wg[:, cols], preferred_element_type=F32)
            up = jnp.dot(x, wu[:, cols], preferred_element_type=F32)
            back = jnp.dot(load(xc, rows, every), wdt[:, cols], preferred_element_type=F32)
            sig = jax.nn.sigmoid(gate)
            active = gate * sig
            hidden = (active * up).astype(BF16)
            store(hid, cols, hidden)
            route = route + jnp.sum(hidden.astype(F32) * back, axis=1, keepdims=True)
            scaled = weight * back
            das.append((scaled * up * sig * (1.0 + gate * (1.0 - sig))).astype(BF16))
            dbs.append((scaled * active).astype(BF16))
            store(da, cols, das[-1])
            store(db, cols, dbs[-1])
        store(rcol, every, jnp.broadcast_to(route, (count, 128)))
        if between is not None:
            between()
        for at in range(nz):
            cols = pl.ds(2 * at * shard, 2 * shard)
            part = None
            for up_to, (left, right) in enumerate(zip(das, dbs)):
                units = pl.ds(up_to * tile, tile)
                term = jnp.dot(left, wgt[units, cols], preferred_element_type=F32)
                part = term if part is None else part + term
                part = part + jnp.dot(right, wut[units, cols], preferred_element_type=F32)
            part, done = part.astype(BF16), 0
            for b, lower, size in parts:
                for core in range(2):
                    rp[core, at, b, pl.ds(lower, size), :] = part[done:done + size, core * shard:(core + 1) * shard]
                done += size
        for b, lower, size in parts:
            for chunk in range(CHUNKS):
                if not lower <= cuts[chunk] < lower + size:
                    continue
                span = span_of(chunk)
                sem = CHUNKS * orders[id(b)] + chunk
                go(remote(rp.at[1 - k, :, b, span], pr.at[:, b, span], s_rp.at[sem], r_rp.at[sem], p, mate))
        store(sc, every, (weight * load(xc, rows, every).astype(F32)).astype(BF16))

    orders = {id(p): 0, id(px): 1, id(py): 2, id(pd): 3}
    def add_pair(b, chunk):
        span = span_of(chunk)
        sem = CHUNKS * orders[id(b)] + chunk
        arrived(pr.at[:, b, span], s_rp.at[sem], r_rp.at[sem])
        for at in range(nz):
            rp[k, at, b, span, :] = (rp[k, at, b, span, :].astype(F32) + pr[at, b, span, :].astype(F32)).astype(BF16)

    def z_first(b):
        add_pair(b, 0)
        for step in range(1, nz):
            sem = orders[id(b)] * nz + step
            go(remote(
                rp.at[k, (z + step) % nz, b, span_of(0)], zq.at[step, orders[id(b)]],
                s_zf.at[sem], r_zf.at[sem], p, (t + 2 * step) % n_tp,
            ))

    def z_sum(b):
        at, span = orders[id(b)], span_of(0)
        total = rp[k, z, b, span, :].astype(F32)
        for step in range(1, nz):
            sem = at * nz + step
            arrived(zq.at[step, at], s_zf.at[sem], r_zf.at[sem])
            total = total + zq[step, at].astype(F32)
        rp[k, z, b, span, :] = total.astype(BF16)
        if at:
            go(remote(rp.at[k, z, b, span], rq.at[at - 1], s_rq.at[at - 1], r_rq.at[at - 1], b, t))

    def xy_sem(at, kind, chunk):
        return (kind * nz + at) * CHUNKS + chunk

    def first(at, b, kind, other, chunk):
        span = span_of(chunk)
        sem = xy_sem(at, kind, chunk)
        go(remote(rp.at[k, at, b, span], r1.at[at, kind, span], s_xy.at[sem], r_xy.at[sem], other, t))

    def first_near(chunk):
        add_pair(px, chunk)
        add_pair(py, chunk)
        for at in range(hz):
            first(at, px, 0, px, chunk)
            first(hz + at, py, 0, py, chunk)

    def first_pd(chunks):
        for chunk in chunks:
            add_pair(pd, chunk)
            for at in range(hz):
                first(at, pd, 1, px, chunk)
                first(hz + at, pd, 1, py, chunk)

    def second(at, b, other, chunk):
        span = span_of(chunk)
        sem = xy_sem(at, 1, chunk)
        arrived(r1.at[at, 1, span], s_xy.at[sem], r_xy.at[sem])
        rp[k, at, b, span, :] = (rp[k, at, b, span, :].astype(F32) + r1[at, 1, span, :].astype(F32)).astype(BF16)
        sem = xy_sem(at, 2, chunk)
        go(remote(rp.at[k, at, b, span], r2.at[at, span], s_xy.at[sem], r_xy.at[sem], other, t))

    def take_near(part):
        for at, other in enumerate((px, py)):
            mine = xc.at[other, half_rows(1 - k, part)]
            sem = 4 + 2 * part + at
            arrived(mine, s_fwd.at[sem], r_fwd.at[sem])
            go(remote(mine, mine, s_pair.at[sem], r_pair.at[sem], p, mate))

    def wait_near(part):
        for at, other in enumerate((px, py)):
            sem = 4 + 2 * part + at
            arrived(xc.at[other, half_rows(k, part)], s_pair.at[sem], r_pair.at[sem])

    def compute_near(group, between=None):
        lower, size = groups[group]
        compute([(px, lower, size), (py, lower, size)], between)

    for at in range(width // 512):
        for to in range(hidden_units // 256):
            a, b = pl.ds(at * 512, 512), pl.ds(to * 256, 256)
            wgt[b, a] = wg[a, b].T
            wut[b, a] = wu[a, b].T
            wdt[a, b] = wd[b, a].T
    compute([(p, 0, rows)])
    mine = xc.at[pd, piece_rows(1 - k, z)]
    arrived(mine, s_fwd.at[3], r_fwd.at[3])
    for step in range(1, nz):
        go(remote(mine, mine, s_z.at[step], r_z.at[step], p, (t + 2 * step) % n_tp))
    go(remote(mine, mine, s_pair.at[0], r_pair.at[0], p, mate))
    take_near(0)
    for at, other in enumerate((px, py)):
        passed = xc.at[other, sub_rows(1 - k, at * piece, piece)]
        sem = 4 + 2 * PARTS + at
        go(remote(passed, passed, s_fwd.at[sem], r_fwd.at[sem], py if at == 0 else px, t))
    send_near(2)
    send_near(3)
    for chunk in range(1, CHUNKS):
        add_pair(p, chunk)
    arrived(wt.at[pd], s_fwd.at[0], r_fwd.at[0])
    arrived(wt.at[px], s_fwd.at[1], r_fwd.at[1])
    arrived(wt.at[py], s_fwd.at[2], r_fwd.at[2])
    wait_near(0)
    compute_near(0)
    take_near(1)
    for step in range(1, nz):
        mine = xc.at[pd, piece_rows(1 - k, (z - step + nz) % nz)]
        arrived(mine, s_z.at[step], r_z.at[step])
        go(remote(mine, mine, s_pair.at[step], r_pair.at[step], p, mate))
    for at in range(2):
        sem = 4 + 2 * PARTS + at
        passed = xc.at[pd, sub_rows(1 - k, at * piece, piece)]
        arrived(passed, s_fwd.at[sem], r_fwd.at[sem])
        go(remote(passed, passed, s_pair.at[sem], r_pair.at[sem], p, mate))
    z_first(px)
    z_first(py)
    for at in range(2):
        sem = 4 + 2 * PARTS + at
        arrived(xc.at[pd, sub_rows(k, at * piece, piece)], s_pair.at[sem], r_pair.at[sem])
    for step in range(nz):
        arrived(xc.at[pd, piece_rows(k, (z - step + nz) % nz)], s_pair.at[step], r_pair.at[step])

    def pass_on():
        take_near(2)
        z_first(p)

    compute([(pd, 0, rows)], pass_on)
    wait_near(1)
    wait_near(2)

    def send_far():
        first_pd(range(1, CHUNKS))
        z_first(pd)

    compute_near(1, send_far)
    take_near(3)
    first_near(1)

    def second_both(chunk):
        for at in range(hz):
            second(at, py, py, chunk)
            second(hz + at, px, px, chunk)

    wait_near(3)
    compute_near(2, lambda: second_both(1))

    def wide(ref, lower, count, cols):
        got = ref[:, pl.ds(lower, count), cols]
        return got.reshape(n_ep * count, got.shape[2])

    def up_grads(*slices):
        for at in slices:
            cols = pl.ds(at * (width // 8), width // 8)
            left = wide(xc, 0, rows, cols)
            for grads, out in ((da, gg), (db, gu)):
                out[cols, :] = lax.dot_general(
                    left, wide(grads, 0, rows, slice(None)), tn, preferred_element_type=F32
                ).astype(BF16)

    def third(chunk):
        span = span_of(chunk)
        for at in range(nz):
            for kind, ref in ((0, r1.at[at, 0, span]), (2, r2.at[at, span])):
                sem = xy_sem(at, kind, chunk)
                arrived(ref, s_xy.at[sem], r_xy.at[sem])
            mine = rp[k, at, p, span, :].astype(F32) + r1[at, 0, span, :].astype(F32) + r2[at, span, :].astype(F32)
            rp[k, at, p, span, :] = mine.astype(BF16)
        for step in range(1, nz):
            sem = (1 + chunk) * nz + step
            go(remote(rp.at[k, (z + step) % nz, p, span], zr.at[step, span], s_z.at[sem], r_z.at[sem], p, (t + 2 * step) % n_tp))

    def send_route():
        for b in range(n_ep):
            rm[b:b + 1, :] = rcol[b].T[0:1, :]
        for step in range(1, n_tp):
            go(remote(rm, rr.at[step], s_rt.at[step], r_rt.at[step], p, (t + step) % n_tp))

    def return_route():
        total = rm[...]
        for step in range(1, n_tp):
            arrived(rr.at[step], s_rt.at[step], r_rt.at[step])
            total = total + rr[step]
        ra[...] = total
        for at, other in enumerate((px, py, pd)):
            go(remote(ra, rb.at[at], s_rt.at[n_tp + at], r_rt.at[n_tp + at], other, t))

    send_route()
    up_grads(0, 1)
    for chunk in range(2, CHUNKS):
        first_near(chunk)
        second_both(chunk)
    third(1)
    up_grads(2, 3)
    z_sum(p)
    z_sum(px)
    z_sum(py)
    z_sum(pd)
    up_grads(4)
    third(2)
    up_grads(5)
    third(3)
    return_route()
    up_grads(6, 7)

    index = lax.broadcasted_iota(jnp.int32, rm.shape, 0)
    result = jnp.zeros(rm.shape, F32)
    for at, other in enumerate((px, py, pd, p)):
        if at < 3:
            arrived(rb.at[at], s_rt.at[n_tp + at], r_rt.at[n_tp + at])
        got = rb[at] if at < 3 else ra[...]
        row = jnp.sum(jnp.where(index == p, got, 0.0), axis=0, keepdims=True)
        result = result + jnp.where(index == other, row, 0.0)
    for choice in range(routes_ref.shape[0]):
        hit = routes_ref[choice:choice + 1, :] == experts
        rt_ref[choice:choice + 1, :] = jnp.sum(jnp.where(hit, result[:, 0:rows], 0.0), axis=0, keepdims=True)

    total = rp[k, z, p, span_of(0), :].astype(F32)
    for at in range(3):
        arrived(rq.at[at], s_rq.at[at], r_rq.at[at])
        total = total + rq[at].astype(F32)
    gt_ref[span_of(0), :] = total.astype(BF16)
    for chunk in range(1, CHUNKS):
        span = span_of(chunk)
        total = rp[k, z, p, span, :].astype(F32)
        for step in range(1, nz):
            sem = (1 + chunk) * nz + step
            arrived(zr.at[step, span], s_z.at[sem], r_z.at[sem])
            total = total + zr[step, span, :].astype(F32)
        gt_ref[span, :] = total.astype(BF16)
    for copy in sends:
        copy.wait_send()


def write_kernel(gt, rt, gg, gu, hid, sc, gt_hbm, rt_hbm, gg_hbm, gu_hbm, gd_hbm, gd, sem):
    pairs = ((gt, gt_hbm), (rt, rt_hbm), (gg, gg_hbm), (gu, gu_hbm))
    copies = [pltpu.make_async_copy(left, right, sem.at[at]) for at, (left, right) in enumerate(pairs)]
    units, width = gd.shape
    merged = hid.shape[0] * hid.shape[1]
    for copy in copies:
        copy.start()
    for at in range(4):
        cols = pl.ds(at * (width // 4), width // 4)
        gd[:, cols] = lax.dot_general(
            hid[...].reshape(merged, units), sc[:, :, cols].reshape(merged, width // 4),
            (((0,), (0,)), ((), ())), preferred_element_type=F32,
        ).astype(BF16)
        copies.append(pltpu.make_async_copy(gd.at[:, cols], gd_hbm.at[:, cols], sem.at[4 + at]))
        copies[-1].start()
    for copy in copies:
        copy.wait()


def fused(n_ep, n_tp, tokens, cotangent, routes, route_weight, gate_weight, up_weight, down_weight):
    rows, width = tokens.shape
    units = gate_weight.shape[2]
    nz = n_tp // 2
    shard = width // n_tp
    hbm, vmem = pl.BlockSpec(memory_space=pltpu.HBM), pl.BlockSpec(memory_space=pltpu.VMEM)
    dma = pltpu.SemaphoreType.DMA
    results = pl.pallas_call(
        functools.partial(step_kernel, n_ep, n_tp),
        out_shape=(
            jax.ShapeDtypeStruct((rows, shard), BF16),
            jax.ShapeDtypeStruct((routes.shape[1], rows), F32),
            jax.ShapeDtypeStruct((width, units), BF16),
            jax.ShapeDtypeStruct((width, units), BF16),
            jax.ShapeDtypeStruct((n_ep, rows, units), BF16),
            jax.ShapeDtypeStruct((n_ep, rows, width), BF16),
        ),
        in_specs=[hbm] * 7,
        out_specs=(vmem,) * 6,
        scratch_shapes=[
            pltpu.VMEM((routes.shape[1], rows), jnp.int32),
            pltpu.VMEM((routes.shape[1], rows), F32),
            pltpu.VMEM((units, width), BF16),
            pltpu.VMEM((units, width), BF16),
            pltpu.VMEM((width, units), BF16),
            pltpu.VMEM((n_ep, 2 * rows, width), BF16),
            pltpu.VMEM((n_ep, 8, LANES), F32),
            pltpu.VMEM((width, units), BF16),
            pltpu.VMEM((width, units), BF16),
            pltpu.VMEM((units, width), BF16),
            pltpu.VMEM((n_ep, rows, units), BF16),
            pltpu.VMEM((n_ep, rows, units), BF16),
            pltpu.VMEM((2, nz, n_ep, rows, shard), BF16),
            pltpu.VMEM((nz, n_ep, rows, shard), BF16),
            pltpu.VMEM((nz, 2, rows, shard), BF16),
            pltpu.VMEM((nz, rows, shard), BF16),
            pltpu.VMEM((nz, rows, shard), BF16),
            pltpu.VMEM((n_ep, LANES, 128), F32),
            pltpu.VMEM((8, LANES), F32),
            pltpu.VMEM((n_tp, 8, LANES), F32),
            pltpu.VMEM((8, LANES), F32),
            pltpu.VMEM((3, 8, LANES), F32),
            pltpu.VMEM((nz, n_ep, 2 * (rows // (nz + 2)), shard), BF16),
            pltpu.VMEM((3, 2 * (rows // (nz + 2)), shard), BF16),
            dma((n_ep * nz,)),
            dma((n_ep * nz,)),
            dma((3,)),
            dma((3,)),
            dma((7,)),
            dma((6 + 2 * PARTS,)),
            dma((6 + 2 * PARTS,)),
            dma((6 + 2 * PARTS,)),
            dma((6 + 2 * PARTS,)),
            dma((n_ep * CHUNKS,)),
            dma((n_ep * CHUNKS,)),
            dma((3 * nz * CHUNKS,)),
            dma((3 * nz * CHUNKS,)),
            dma(((1 + CHUNKS) * nz,)),
            dma(((1 + CHUNKS) * nz,)),
            dma((n_tp + 3,)),
            dma((n_tp + 3,)),
        ],
        compiler_params=pltpu.CompilerParams(
            collective_id=0, has_side_effects=True, vmem_limit_bytes=VLIM * 1024 * 1024
        ),
    )(*(pltpu.with_memory_space_constraint(array, pltpu.HBM) for array in (
        tokens, cotangent, routes.T, route_weight.T, gate_weight[0], up_weight[0], down_weight[0]
    )))
    grad_tokens, by_choice, grad_gate, grad_up, grad_down = pl.pallas_call(
        write_kernel,
        out_shape=tuple(jax.ShapeDtypeStruct(array.shape, array.dtype) for array in results[:4])
        + (jax.ShapeDtypeStruct((units, width), BF16),),
        in_specs=[vmem] * 6,
        out_specs=(hbm,) * 5,
        scratch_shapes=[pltpu.VMEM((units, width), BF16), dma((8,))],
        compiler_params=pltpu.CompilerParams(vmem_limit_bytes=8 * 1024 * 1024),
    )(*results)
    grad_route = by_choice.T
    return grad_tokens, grad_route, grad_gate[None], grad_up[None], grad_down[None]


def body(mesh, *arrays):
    n_ep, n_tp = mesh.shape["ep"], mesh.shape["tp"]
    rows, width = arrays[0].shape
    experts, _, units = arrays[4].shape
    capacity = 2 * rows * arrays[2].shape[1] // (experts * n_ep)
    fits = (
        n_ep == 4 and experts == 1 and n_tp == 8 and capacity >= rows and rows <= LANES
        and width % (n_tp * 128) == 0 and width % 512 == 0 and units % 256 == 0
        and units >= 512 and width % 1024 == 0 and rows % (16 * (n_tp // 2 + 2)) == 0
    )
    return fused(n_ep, n_tp, *arrays) if fits else shards(*arrays)


def solution(mesh):
    return jax.shard_map(
        functools.partial(body, mesh),
        mesh=mesh,
        in_specs=(
            P("ep", None),
            P("ep", None),
            P("ep", None),
            P("ep", None),
            P("ep", None, "tp"),
            P("ep", None, "tp"),
            P("ep", "tp", None),
        ),
        out_specs=(
            P("ep", "tp"),
            P("ep", None),
            P("ep", None, "tp"),
            P("ep", None, "tp"),
            P("ep", "tp", None),
        ),
        check_vma=False,
    )
```
